256 devices in a mesh: sp: 64 (over z, x, core), tp: 4 (over y).
Axes of the slice: x: 4, y: 4, z: 8, core: 2. Of those that a mesh axis runs over, the one named last changes fastest.
Arguments:
- residual: bfloat16 [8192, 2048], P(('sp', 'tp')), may hold values from -6 to 6
- query_first: bfloat16 [8192, 1024], P('sp', 'tp'), may hold values from -200 to 200
- key_first: bfloat16 [8192, 1024], P('sp', 'tp'), may hold values from -200 to 200
- query_second: bfloat16 [8192, 1024], P('sp', 'tp'), may hold values from -200 to 200
- key_second: bfloat16 [8192, 1024], P('sp', 'tp'), may hold values from -200 to 200
- values: bfloat16 [8192, 2048], P('sp', 'tp'), may hold values from -6 to 6
- lambda_weight: float32 [16], P('tp'), may hold values from 0.3 to 0.8
- head_gain: float32 [128], replicated, may hold values from 0.1 to 1.9
- out_weight: bfloat16 [2048, 2048], P('sp', 'tp'), may hold values from -0.125 to 0.125
- norm_gain: float32 [2048], replicated, may hold values from 0.1 to 1.9
- gate_weight: bfloat16 [2048, 5632], P(None, 'tp'), may hold values from -0.125 to 0.125
- up_weight: bfloat16 [2048, 5632], P(None, 'tp'), may hold values from -0.125 to 0.125
- down_weight: bfloat16 [2048, 5632], P('sp', 'tp'), may hold values from -0.078125 to 0.078125
Outputs:
- layer_out: bfloat16 [8192, 2048], P(('sp', 'tp'))
The draws below stay inside these ranges and needn't reach their ends.
All inputs are finite; a program needn't handle non-finite values.
Results may differ from the reference program's by a relative error of at most 0.017.
Values may be sent and summed in bfloat16 or wider, within the bound.
A program may use at most 128 MiB of HBM per device.

```python
import jax
import jax.numpy as jnp
from jax import lax

D = 2048
HEADS = 16
HD = 64
VD = 128
FF = 5632
TOKENS = 8192
N_TP = 4


def plant_pair(key, which):
    spread = 1.32
    key_rows = jax.random.normal(jax.random.fold_in(key, 101 + which), (TOKENS, HEADS * HD), jnp.float32) * spread
    key_rows = jnp.clip(key_rows, -6.0 * spread, 6.0 * spread)
    queries = jax.random.normal(jax.random.fold_in(key, 201 + which), (TOKENS, HEADS * HD), jnp.float32) * spread
    queries = jnp.clip(queries, -6.0 * spread, 6.0 * spread)
    return (queries, key_rows)


def draw_query_first(key, part):
    return plant_pair(key, 0)[0].astype(jnp.bfloat16)


def draw_key_first(key, part):
    return plant_pair(key, 0)[1].astype(jnp.bfloat16)


def draw_query_second(key, part):
    return plant_pair(key, 1)[0].astype(jnp.bfloat16)


def draw_key_second(key, part):
    return plant_pair(key, 1)[1].astype(jnp.bfloat16)


def shard_levels(rng, shape, cuts, low, high):
    def one(axis_at, blocks):
        steps = jax.random.uniform(jax.random.fold_in(jax.random.fold_in(rng, 6), axis_at), (blocks,), jnp.float32, low / len(cuts), high / len(cuts))
        return jnp.repeat(jnp.exp(steps), shape[axis_at] // blocks).reshape((-1,) + (1,) * (len(shape) - axis_at - 1))

    level = one(*cuts[0])
    for cut in cuts[1:]:
        level = level * one(*cut)
    return level


def normal_values(stream_key, extent, deviation, reach, cuts=(), held_as=jnp.bfloat16):
    loudness = shard_levels(stream_key, extent, cuts, -0.22, 0.18) if cuts else 1.0
    values = jax.random.normal(stream_key, extent, jnp.float32) * deviation * loudness
    return jnp.minimum(jnp.maximum(values, -reach), reach).astype(held_as)


def setup_inputs(seed: int = 0) -> dict:
    arg_keys = jax.random.split(jax.random.key(seed), 14)
    residual = normal_values(arg_keys[0], (TOKENS, D), 1.0, 6.0, ((0, 256),))
    query_first = draw_query_first(jax.random.fold_in(arg_keys[13], 71), 0)
    key_first = draw_key_first(jax.random.fold_in(arg_keys[13], 71), 0)
    query_second = draw_query_second(jax.random.fold_in(arg_keys[13], 71), 0)
    key_second = draw_key_second(jax.random.fold_in(arg_keys[13], 71), 0)
    values = normal_values(arg_keys[5], (TOKENS, HEADS * VD), 1.0, 6.0, ((0, 64), (1, 4)))
    lambda_weight = jnp.clip(0.3 + 0.5 * jax.random.uniform(arg_keys[6], (HEADS,), jnp.float32) ** shard_levels(arg_keys[6], (HEADS,), ((0, 4),), -0.2, 0.2), 0.3, 0.8)
    head_gain = jnp.clip(1.0 + 0.18 * jax.random.normal(arg_keys[7], (VD,), jnp.float32), 0.1, 1.9)
    out_weight = normal_values(arg_keys[8], (D, HEADS * VD), (HEADS * VD) ** -0.5, 0.125, ((0, 64), (1, 4)))
    norm_gain = jnp.clip(1.0 + 0.18 * jax.random.normal(arg_keys[9], (D,), jnp.float32), 0.1, 1.9)
    gate_weight = normal_values(arg_keys[10], (D, FF), D ** -0.5, 0.125, ((1, 4),))
    up_weight = normal_values(arg_keys[11], (D, FF), D ** -0.5, 0.125, ((1, 4),))
    down_weight = normal_values(arg_keys[12], (D, FF), FF ** -0.5, 0.078125, ((0, 64), (1, 4)))
    return {"residual": residual, "query_first": query_first, "key_first": key_first, "query_second": query_second, "key_second": key_second, "values": values, "lambda_weight": lambda_weight, "head_gain": head_gain, "out_weight": out_weight, "norm_gain": norm_gain, "gate_weight": gate_weight, "up_weight": up_weight, "down_weight": down_weight}


epsilon = 1e-06

def one_map(queries, key_rows, value_rows):
    scores = jnp.dot(queries, key_rows.T, preferred_element_type=jnp.float32) * queries.shape[-1] ** (-0.5)
    shifted = jnp.exp(scores - lax.optimization_barrier(jnp.max(scores, axis=-1, keepdims=True)))
    totals = lax.optimization_barrier(jnp.sum(shifted, axis=-1, keepdims=True))
    product = jnp.dot(shifted.astype(jnp.bfloat16), value_rows, preferred_element_type=jnp.float32)
    return product / totals

def attend_head(inputs, head_gain):
    query_one, key_one, query_two, key_two, value_rows, weight = inputs
    first_map = one_map(query_one, key_one, value_rows)
    second_map = one_map(query_two, key_two, value_rows)
    difference = first_map - weight * second_map
    scaled = difference * lax.rsqrt(lax.optimization_barrier(jnp.mean(difference * difference, axis=-1, keepdims=True)) + epsilon)
    return (scaled * head_gain).astype(jnp.bfloat16)

def reference(residual, query_first, key_first, query_second, key_second, values, lambda_weight, head_gain, out_weight, norm_gain, gate_weight, up_weight, down_weight):
    length = query_first.shape[0]

    def split_heads(array, entries):
        return array.reshape(length, HEADS, entries).transpose(1, 0, 2)
    stacked = (split_heads(query_first, HD), split_heads(key_first, HD), split_heads(query_second, HD), split_heads(key_second, HD), split_heads(values, VD), lambda_weight)
    heads_out = lax.map(lambda inputs: attend_head(inputs, head_gain), stacked)
    attended = heads_out.transpose(1, 0, 2).reshape(length, HEADS * VD)
    group_width = HEADS * VD // N_TP
    projected = jnp.zeros((length, D), jnp.float32)
    for member in range(N_TP):
        columns = slice(member * group_width, (member + 1) * group_width)
        partial_value = lax.dot_general(attended[:, columns], out_weight[:, columns], (((1,), (1,)), ((), ())), preferred_element_type=jnp.float32)
        projected = projected + lax.optimization_barrier(partial_value.astype(jnp.bfloat16)).astype(jnp.float32)
    after_attention = (residual.astype(jnp.float32) + projected).astype(jnp.bfloat16)
    stream = after_attention.astype(jnp.float32)
    normed = (stream * lax.rsqrt(lax.optimization_barrier(jnp.mean(stream * stream, axis=-1, keepdims=True)) + epsilon) * norm_gain).astype(jnp.bfloat16)
    hidden_width = FF // N_TP
    feed_sum = jnp.zeros((length, D), jnp.float32)
    for member in range(N_TP):
        columns = slice(member * hidden_width, (member + 1) * hidden_width)
        gate_part = jnp.dot(normed, gate_weight[:, columns], preferred_element_type=jnp.float32)
        up_part = jnp.dot(normed, up_weight[:, columns], preferred_element_type=jnp.float32)
        hidden = (jax.nn.silu(gate_part) * up_part).astype(jnp.bfloat16)
        partial_value = lax.dot_general(hidden, down_weight[:, columns], (((1,), (1,)), ((), ())), preferred_element_type=jnp.float32)
        feed_sum = feed_sum + lax.optimization_barrier(partial_value.astype(jnp.bfloat16)).astype(jnp.float32)
    return (stream + feed_sum).astype(jnp.bfloat16)
```

```python
import functools
import math

import jax
import jax.numpy as jnp
from jax import lax
from jax.experimental import pallas as pl
from jax.experimental.pallas import tpu as pltpu
from jax.sharding import PartitionSpec as P

EPS = 1e-06
MESH = pl.DeviceIdType.MESH
NX = 4
NC = 2
F32 = jnp.float32
BF16 = jnp.bfloat16


def dot_nt(a, b):
    return lax.dot_general(a, b, (((1,), (1,)), ((), ())), preferred_element_type=F32)


def attention_kernel(
    nz,
    n_tp,
    q1_ref,
    q2_ref,
    k1_ref,
    k2_ref,
    v_ref,
    lam_ref,
    gain_ref,
    att_ref,
    packq,
    packkv,
    qrecv,
    qs,
    kv,
    acc,
    mx,
    tot,
    asend,
    arecv,
    xs_sem,
    xr_sem,
    rs_sem,
    rr_sem,
    ls_sem,
    lr_sem,
    ds_sem,
    dr_sem,
    as_sem,
    ar_sem,
):
    sp = lax.axis_index("sp")
    tp = lax.axis_index("tp")
    z = sp // (NX * NC)
    x = (sp // NC) % NX
    c = sp % NC
    tokens = q1_ref.shape[0]
    rows = NX * tokens
    half = rows // 2
    steps = nz - 1

    def dev(zz, xx, cc):
        return ((zz * NX + xx) * NC + cc, tp)

    z_up = (z + 1) % nz
    z_dn = (z + nz - 1) % nz
    peers = [dev(z, (x + d) % NX, c) for d in range(1, NX)]
    peers += [dev(z_up, x, c), dev(z_dn, x, c), dev(z, x, 1 - c)]
    barrier = pltpu.get_barrier_semaphore()
    for p in peers:
        pl.semaphore_signal(barrier, inc=1, device_id=p, device_id_type=MESH)

    low = lax.broadcasted_iota(jnp.int32, (tokens, 128), 1) < 64

    def joined(first, second, j):
        a = first[:, 128 * (j // 2) : 128 * (j // 2) + 128].astype(F32)
        b = second[:, 128 * (j // 2) : 128 * (j // 2) + 128].astype(F32)
        if j % 2 == 0:
            b = pltpu.roll(b, 64, 1)
        else:
            a = pltpu.roll(a, 64, 1)
        return jnp.where(low, a, b).astype(BF16)

    for j in range(NX):
        packkv[j, 0] = joined(k1_ref, k2_ref, j)
        packkv[j, 1] = v_ref[:, 128 * j : 128 * j + 128]
        packq[j] = joined(q1_ref, q2_ref, j)
    mine = z * NC + c
    my_rows = pl.ds(pl.multiple_of(x * tokens, tokens), tokens)
    kv[mine, :, my_rows, :] = packkv[x]
    qrecv[my_rows, :] = packq[x]
    acc[...] = jnp.zeros_like(acc)
    tot[...] = jnp.zeros_like(tot)
    mx[...] = jnp.full(mx.shape, -3e38, F32)
    pl.semaphore_wait(barrier, len(peers))

    x_copies = []
    for d in range(1, NX):
        to = (x + d) % NX
        x_copies.append(
            pltpu.make_async_remote_copy(
                src_ref=packkv.at[to],
                dst_ref=kv.at[mine, :, my_rows, :],
                send_sem=xs_sem.at[d - 1],
                recv_sem=xr_sem.at[d - 1],
                device_id=dev(z, to, c),
                device_id_type=MESH,
            )
        )
    for d in range(1, NX):
        to = (x + d) % NX
        x_copies.append(
            pltpu.make_async_remote_copy(
                src_ref=packq.at[to],
                dst_ref=qrecv.at[my_rows, :],
                send_sem=xs_sem.at[NX - 1 + d - 1],
                recv_sem=xr_sem.at[NX - 1 + d - 1],
                device_id=dev(z, to, c),
                device_id_type=MESH,
            )
        )
    for copy in x_copies:
        copy.start()

    def piece(slot, which):
        off = pl.multiple_of(which * half, half)
        return kv.at[slot, :, pl.ds(off, half), :]

    def up_copy(slot, which, index):
        return pltpu.make_async_remote_copy(
            src_ref=piece(slot, which),
            dst_ref=piece(slot, which),
            send_sem=rs_sem.at[index],
            recv_sem=rr_sem.at[index],
            device_id=dev(z_up, x, c),
            device_id_type=MESH,
        )

    def down_copy(slot, which, index):
        return pltpu.make_async_remote_copy(
            src_ref=piece(slot, which),
            dst_ref=piece(slot, which),
            send_sem=ls_sem.at[index],
            recv_sem=lr_sem.at[index],
            device_id=dev(z_dn, x, c),
            device_id_type=MESH,
        )

    def side_copy(slot, which, index):
        return pltpu.make_async_remote_copy(
            src_ref=piece(slot, which),
            dst_ref=piece(slot, which),
            send_sem=ds_sem.at[index],
            recv_sem=dr_sem.at[index],
            device_id=dev(z, x, 1 - c),
            device_id_type=MESH,
        )

    def from_below(j, core):
        d = (j + 2) // 2
        which = jnp.where(j < 0, 0, (j + 2) % 2)
        return ((z + nz - d) % nz) * NC + core, which

    def from_above(j, core):
        d = (j + 2) // 2
        which = jnp.where((j < 0) | (j == steps - 1), 1, (j + 2) % 2)
        return ((z + d) % nz) * NC + core, which

    for copy in x_copies[: NX - 1]:
        copy.wait_recv()
    for h in range(2):
        up_copy(mine, h, h).start()
        down_copy(mine, h, h).start()
    for h in range(2):
        side_copy(mine, h, h).start()
    for copy in x_copies[NX - 1 :]:
        copy.wait_recv()
    lane = lax.broadcasted_iota(jnp.int32, (rows, 128), 1) < 64
    queries = qrecv[...].astype(F32)
    qs[0:rows, :] = jnp.where(lane, queries, 0.0).astype(BF16)
    qs[rows : 2 * rows, :] = jnp.where(lane, 0.0, queries).astype(BF16)

    scale = 64 ** (-0.5) * math.log2(math.e)
    tile = min(256, 2 * rows)

    def attend(blocks):
        def body(r, carry):
            at = pl.ds(pl.multiple_of(r * tile, tile), tile)
            q = qs[at, :]
            scores = []
            for slot, which in blocks:
                off = pl.multiple_of(which * half, half)
                scores.append(dot_nt(q, kv[slot, 0, pl.ds(off, half), :]))
            old = mx[at, :]
            top = None
            for s in scores:
                for lo in range(0, half, 128):
                    part = s[:, lo : lo + 128]
                    top = part if top is None else jnp.maximum(top, part)
            new = jnp.maximum(old, jnp.max(top, axis=1, keepdims=True))
            factor = jnp.exp2((old - new) * scale)
            total = tot[at, :] * factor
            product = acc[at, :] * factor
            for (slot, which), s in zip(blocks, scores):
                off = pl.multiple_of(which * half, half)
                parts = []
                for lo in range(0, half, 128):
                    part = jnp.exp2((s[:, lo : lo + 128] - new) * scale)
                    total = total + part
                    parts.append(part.astype(BF16))
                p = jnp.concatenate(parts, axis=1)
                product = product + jnp.dot(
                    p, kv[slot, 1, pl.ds(off, half), :], preferred_element_type=F32
                )
            mx[at, :] = new
            tot[at, :] = total
            acc[at, :] = product
            return carry

        lax.fori_loop(0, 2 * rows // tile, body, 0)

    attend([(mine, 0), (mine, 1)])

    def step(i, carry):
        below, below_half = from_below(i, c)
        above, above_half = from_above(i, c)
        up_copy(below, below_half, i).wait_recv()
        down_copy(above, above_half, i).wait_recv()

        @pl.when(i < steps - 2)
        def _():
            up_copy(below, below_half, i + 2).start()

        @pl.when((i < steps - 3) | (i == steps - 2))
        def _():
            down_copy(above, above_half, jnp.minimum(i + 2, steps - 1)).start()

        side_copy(below, below_half, i + 2 + 0 * below).start()
        side_copy(above, above_half, steps + i + 2).start()
        other_b, other_bh = from_below(i - 1, 1 - c)
        other_a, other_ah = from_above(i - 1, 1 - c)
        b_index = jnp.where(i == 0, 0, i + 1)
        a_index = jnp.where(i == 0, 1, steps + i + 1)
        side_copy(other_b, other_bh, b_index).wait_recv()
        side_copy(other_a, other_ah, a_index).wait_recv()
        attend([(below, below_half), (above, above_half), (other_b, other_bh), (other_a, other_ah)])
        return carry

    lax.fori_loop(0, steps, step, 0)
    other_b, other_bh = from_below(steps - 1, 1 - c)
    other_a, other_ah = from_above(steps - 1, 1 - c)
    side_copy(other_b, other_bh, steps + 1).wait_recv()
    side_copy(other_a, other_ah, 2 * steps + 1).wait_recv()
    attend([(other_b, other_bh), (other_a, other_ah)])

    weight = lam_ref[x]
    for j in range(NX):
        a, b = j * tokens, rows + j * tokens
        first = acc[a : a + tokens, :] / jnp.sum(tot[a : a + tokens, :], axis=1, keepdims=True)
        second = acc[b : b + tokens, :] / jnp.sum(tot[b : b + tokens, :], axis=1, keepdims=True)
        diff = first - weight * second
        normal = diff * lax.rsqrt(jnp.mean(diff * diff, axis=1, keepdims=True) + EPS)
        asend[j] = (normal * gain_ref[...]).astype(BF16)

    my_cols = pl.ds(pl.multiple_of(x * 128, 128), 128)
    a_copies = []
    for d in range(1, NX):
        to = (x + d) % NX
        copy = pltpu.make_async_remote_copy(
            src_ref=asend.at[to],
            dst_ref=arecv.at[:, my_cols],
            send_sem=as_sem.at[d - 1],
            recv_sem=ar_sem.at[d - 1],
            device_id=dev(z, to, c),
            device_id_type=MESH,
        )
        copy.start()
        a_copies.append(copy)
    arecv[:, my_cols] = asend[x]
    for copy in x_copies:
        copy.wait_send()
    for h in range(steps):
        up_copy(mine, 0, h).wait_send()
        down_copy(mine, 0, h).wait_send()
    for h in range(2 * steps + 2):
        side_copy(mine, 0, h).wait_send()
    for copy in a_copies:
        copy.wait()
    att_ref[...] = arecv[...]


def attention(nz, n_tp, q1, q2, k1, k2, v, lam, gain):
    tokens = q1.shape[0]
    rows = NX * tokens
    steps = nz - 1
    vmem = pl.BlockSpec(memory_space=pltpu.VMEM)
    dma = pltpu.SemaphoreType.DMA
    flops = 2 * 2 * 2 * rows * nz * NC * rows * 128
    return pl.pallas_call(
        functools.partial(attention_kernel, nz, n_tp),
        out_shape=jax.ShapeDtypeStruct((tokens, NX * 128), BF16),
        in_specs=[vmem] * 5 + [pl.BlockSpec(memory_space=pltpu.SMEM), vmem],
        out_specs=vmem,
        scratch_shapes=[
            pltpu.VMEM((NX, tokens, 128), BF16),
            pltpu.VMEM((NX, 2, tokens, 128), BF16),
            pltpu.VMEM((rows, 128), BF16),
            pltpu.VMEM((2 * rows, 128), BF16),
            pltpu.VMEM((nz * NC, 2, rows, 128), BF16),
            pltpu.VMEM((2 * rows, 128), F32),
            pltpu.VMEM((2 * rows, 128), F32),
            pltpu.VMEM((2 * rows, 128), F32),
            pltpu.VMEM((NX, tokens, 128), BF16),
            pltpu.VMEM((tokens, NX * 128), BF16),
            dma((2 * (NX - 1),)),
            dma((2 * (NX - 1),)),
            dma((steps,)),
            dma((steps,)),
            dma((steps,)),
            dma((steps,)),
            dma((2 * steps + 2,)),
            dma((2 * steps + 2,)),
            dma((NX - 1,)),
            dma((NX - 1,)),
        ],
        compiler_params=pltpu.CompilerParams(
            collective_id=0, has_side_effects=True, vmem_limit_bytes=40 * 2**20
        ),
        cost_estimate=pl.CostEstimate(flops=20 * flops, bytes_accessed=2**22, transcendentals=0),
        name="attend",
    )(q1, q2, k1, k2, v, lam, gain.reshape(1, 128))


def feed_kernel(
    n_tp,
    att_ref,
    w_ref,
    res_ref,
    gain_ref,
    gate_ref,
    up_ref,
    out_ref,
    wv,
    gv,
    uv,
    psend,
    precv,
    after,
    nsend,
    shard,
    hid,
    dsend,
    drecv,
    load_sem,
    ps_sem,
    pr_sem,
    ns_sem,
    nr_sem,
    ds_sem,
    dr_sem,
):
    sp = lax.axis_index("sp")
    tp = lax.axis_index("tp")
    loads = [
        pltpu.make_async_copy(w_ref, wv, load_sem.at[0]),
        pltpu.make_async_copy(gate_ref, gv, load_sem.at[1]),
        pltpu.make_async_copy(up_ref, uv, load_sem.at[2]),
    ]
    for load in loads:
        load.start()
    barrier = pltpu.get_barrier_semaphore()
    for d in range(1, n_tp):
        pl.semaphore_signal(
            barrier, inc=1, device_id=(sp, (tp + d) % n_tp), device_id_type=MESH
        )
    width = att_ref.shape[1]
    n_rows = res_ref.shape[0]
    features = res_ref.shape[1]
    cols = 512

    def exchange(send, recv, s_sem, r_sem):
        copies = []
        for d in range(1, n_tp):
            to = (tp + d) % n_tp
            copy = pltpu.make_async_remote_copy(
                src_ref=send.at[to],
                dst_ref=recv.at[d - 1],
                send_sem=s_sem.at[d - 1],
                recv_sem=r_sem.at[d - 1],
                device_id=(sp, to),
                device_id_type=MESH,
            )
            copy.start()
            copies.append(copy)
        return copies

    loads[0].wait()

    def project(i, carry):
        at = pl.ds(pl.multiple_of(i * cols, cols), cols)
        part = dot_nt(att_ref[...], wv[at, 0:width]).astype(BF16)
        for t in range(n_tp):
            psend[t, :, at] = part[t * n_rows : (t + 1) * n_rows, :]
        return carry

    lax.fori_loop(0, features // cols, project, 0)
    pl.semaphore_wait(barrier, n_tp - 1)
    copies = exchange(psend, precv, ps_sem, pr_sem)
    total = psend[tp].astype(F32)
    for copy in copies:
        copy.wait()
    for d in range(n_tp - 1):
        total = total + precv[d].astype(F32)
    summed = (res_ref[...].astype(F32) + total).astype(BF16)
    after[...] = summed
    stream = summed.astype(F32)
    normal = stream * lax.rsqrt(jnp.mean(stream * stream, axis=1, keepdims=True) + EPS)
    normed = (normal * gain_ref[...]).astype(BF16)
    nsend[...] = normed
    my_rows = pl.ds(pl.multiple_of(tp * n_rows, n_rows), n_rows)
    copies = []
    for d in range(1, n_tp):
        copy = pltpu.make_async_remote_copy(
            src_ref=nsend,
            dst_ref=shard.at[my_rows, :],
            send_sem=ns_sem.at[d - 1],
            recv_sem=nr_sem.at[d - 1],
            device_id=(sp, (tp + d) % n_tp),
            device_id_type=MESH,
        )
        copy.start()
        copies.append(copy)
    shard[my_rows, :] = normed
    loads[1].wait()
    loads[2].wait()
    for copy in copies:
        copy.wait()
    hidden_width = gv.shape[1]
    lo = 0
    while lo < hidden_width:
        hi = min(lo + 256, hidden_width)
        gate = jnp.dot(shard[...], gv[:, lo:hi], preferred_element_type=F32)
        up = jnp.dot(shard[...], uv[:, lo:hi], preferred_element_type=F32)
        hid[:, lo:hi] = (gate / (1.0 + jnp.exp(-gate)) * up).astype(BF16)
        lo = hi

    def down(i, carry):
        at = pl.ds(pl.multiple_of(i * cols, cols), cols)
        part = dot_nt(hid[...], wv[at, width : width + hidden_width]).astype(BF16)
        for t in range(n_tp):
            dsend[t, :, at] = part[t * n_rows : (t + 1) * n_rows, :]
        return carry

    lax.fori_loop(0, features // cols, down, 0)
    copies = exchange(dsend, drecv, ds_sem, dr_sem)
    total = dsend[tp].astype(F32)
    for copy in copies:
        copy.wait()
    for d in range(n_tp - 1):
        total = total + drecv[d].astype(F32)
    out_ref[...] = (after[...].astype(F32) + total).astype(BF16)


def feed(n_tp, att, weights, residual, gain, gate, up):
    n_rows, features = residual.shape
    tokens = att.shape[0]
    hidden = gate.shape[1]
    vmem = pl.BlockSpec(memory_space=pltpu.VMEM)
    hbm = pl.BlockSpec(memory_space=pl.ANY)
    dma = pltpu.SemaphoreType.DMA
    return pl.pallas_call(
        functools.partial(feed_kernel, n_tp),
        out_shape=jax.ShapeDtypeStruct((n_rows, features), BF16),
        in_specs=[vmem, hbm, vmem, vmem, hbm, hbm],
        out_specs=vmem,
        scratch_shapes=[
            pltpu.VMEM(weights.shape, BF16),
            pltpu.VMEM(gate.shape, BF16),
            pltpu.VMEM(up.shape, BF16),
            pltpu.VMEM((n_tp, n_rows, features), BF16),
            pltpu.VMEM((n_tp - 1, n_rows, features), BF16),
            pltpu.VMEM((n_rows, features), BF16),
            pltpu.VMEM((n_rows, features), BF16),
            pltpu.VMEM((tokens, features), BF16),
            pltpu.VMEM((tokens, hidden), BF16),
            pltpu.VMEM((n_tp, n_rows, features), BF16),
            pltpu.VMEM((n_tp - 1, n_rows, features), BF16),
            dma((3,)),
            dma((n_tp - 1,)),
            dma((n_tp - 1,)),
            dma((n_tp - 1,)),
            dma((n_tp - 1,)),
            dma((n_tp - 1,)),
            dma((n_tp - 1,)),
        ],
        compiler_params=pltpu.CompilerParams(
            collective_id=1, has_side_effects=True, vmem_limit_bytes=60 * 2**20
        ),
        name="feed",
    )(att, weights, residual, gain.reshape(1, features), gate, up)


def local(nz, n_tp, residual, q1, k1, q2, k2, v, lam, head_gain, out_w, norm_gain, gate, up, down):
    weights = lax.all_gather(jnp.concatenate([out_w, down], axis=1), "sp", axis=0, tiled=True)
    att = attention(nz, n_tp, q1, q2, k1, k2, v, lam, head_gain)
    return feed(n_tp, att, weights, residual, norm_gain, gate, up)


def solution(mesh):
    nz = mesh.shape["sp"] // (NX * NC)
    n_tp = mesh.shape["tp"]
    return jax.shard_map(
        functools.partial(local, nz, n_tp),
        mesh=mesh,
        in_specs=(
            P(("sp", "tp"), None),
            P("sp", "tp"),
            P("sp", "tp"),
            P("sp", "tp"),
            P("sp", "tp"),
            P("sp", "tp"),
            P("tp"),
            P(),
            P("sp", "tp"),
            P(),
            P(None, "tp"),
            P(None, "tp"),
            P("sp", "tp"),
        ),
        out_specs=P(("sp", "tp"), None),
        check_vma=False,
    )
```

```python
import functools
import math

import jax
import jax.numpy as jnp
from jax import lax
from jax.experimental import pallas as pl
from jax.experimental.pallas import tpu as pltpu
from jax.sharding import PartitionSpec as P

EPS = 1e-06
MESH = pl.DeviceIdType.MESH
NX = 4
NC = 2
DOWN_AT = 4
F32 = jnp.float32
BF16 = jnp.bfloat16


def dot_nt(a, b):
    return lax.dot_general(a, b, (((1,), (1,)), ((), ())), preferred_element_type=F32)


def remote(src, dst, send, recv, device):
    return pltpu.make_async_remote_copy(
        src_ref=src,
        dst_ref=dst,
        send_sem=send,
        recv_sem=recv,
        device_id=device,
        device_id_type=MESH,
    )


def kernel(
    nz,
    n_tp,
    res_hbm,
    q1_hbm,
    k1_hbm,
    q2_hbm,
    k2_hbm,
    v_hbm,
    lam_ref,
    hgain_ref,
    outw_hbm,
    ngain_ref,
    gate_hbm,
    up_hbm,
    downw_hbm,
    out_ref,
    res,
    q1,
    k1,
    q2,
    k2,
    v,
    gv,
    uv,
    wo,
    wd,
    packq,
    packkv,
    qrecv,
    qs,
    kv,
    acc,
    mx,
    tot,
    asend,
    arecv,
    psend,
    precv,
    after,
    nsend,
    shard,
    hid,
    dsend,
    drecv,
    load_sem,
    xs_sem,
    xr_sem,
    us_sem,
    ur_sem,
    ls_sem,
    lr_sem,
    ds_sem,
    dr_sem,
    as_sem,
    ar_sem,
    wus_sem,
    wur_sem,
    wls_sem,
    wlr_sem,
    wxs_sem,
    wxr_sem,
    wds_sem,
    wdr_sem,
    ps_sem,
    pr_sem,
    ns_sem,
    nr_sem,
    fs_sem,
    fr_sem,
):
    sp = lax.axis_index("sp")
    tp = lax.axis_index("tp")
    z = sp // (NX * NC)
    x = (sp // NC) % NX
    c = sp % NC
    tokens = q1.shape[0]
    rows = NX * tokens
    steps = NX * (nz - 1) // 2
    mid = nz // 2
    half = NX // 2

    def dev(zz, xx, cc):
        return ((zz * NX + xx) * NC + cc, tp)

    z_up = (z + 1) % nz
    z_dn = (z + nz - 1) % nz
    other = dev(z, x, 1 - c)

    loads = []
    for n, (src, dst) in enumerate(
        (
            (k1_hbm, k1),
            (k2_hbm, k2),
            (v_hbm, v),
            (q1_hbm, q1),
            (q2_hbm, q2),
            (outw_hbm, wo.at[z, x, c]),
            (downw_hbm, wd.at[z, x, c]),
            (gate_hbm, gv),
            (up_hbm, uv),
            (res_hbm, res),
        )
    ):
        load = pltpu.make_async_copy(src, dst, load_sem.at[n])
        load.start()
        loads.append(load)

    peers = [dev(z, (x + d) % NX, c) for d in range(1, NX)]
    peers += [dev(z_up, x, c), dev(z_dn, x, c), other]
    peers += [(sp, (tp + d) % n_tp) for d in range(1, n_tp)]
    barrier = pltpu.get_barrier_semaphore()
    for p in peers:
        pl.semaphore_signal(barrier, inc=1, device_id=p, device_id_type=MESH)

    low = lax.broadcasted_iota(jnp.int32, (tokens, 128), 1) < 64

    def joined(first, second, j):
        a = first[:, 128 * (j // 2) : 128 * (j // 2) + 128].astype(F32)
        b = second[:, 128 * (j // 2) : 128 * (j // 2) + 128].astype(F32)
        if j % 2 == 0:
            b = pltpu.roll(b, 64, 1)
        else:
            a = pltpu.roll(a, 64, 1)
        return jnp.where(low, a, b).astype(BF16)

    mine = z * NC + c
    my_rows = pl.ds(pl.multiple_of(x * tokens, tokens), tokens)
    for load in loads[:3]:
        load.wait()
    for j in range(NX):
        packkv[j, 0] = joined(k1, k2, j)
        packkv[j, 1] = v[:, 128 * j : 128 * j + 128]
    kv[mine, :, my_rows, :] = packkv[x]
    for load in loads[3:5]:
        load.wait()
    for j in range(NX):
        packq[j] = joined(q1, q2, j)
    qrecv[my_rows, :] = packq[x]
    pl.semaphore_wait(barrier, len(peers))

    order = [0, 1, NX - 1] + list(range(2, NX - 1))

    def source(s):
        back = s
        for n, d in enumerate(order):
            back = jnp.where(s == n, d, back)
        return (x + NX - back) % NX

    def piece(slot, s):
        at = pl.multiple_of(source(s) * tokens, tokens)
        return kv.at[slot, :, pl.ds(at, tokens), :]

    def up_copy(slot, s, index):
        part = piece(slot, s)
        return remote(part, part, us_sem.at[index], ur_sem.at[index], dev(z_up, x, c))

    def low_copy(slot, s, index):
        part = piece(slot, s)
        return remote(part, part, ls_sem.at[index], lr_sem.at[index], dev(z_dn, x, c))

    def side_copy(slot, s, index):
        part = piece(slot, s)
        return remote(part, part, ds_sem.at[index], dr_sem.at[index], other)

    def from_below(j, core):
        d = (j + NX) // NX
        s = jnp.where(j < 0, 2 * (j + half), (j + NX) % NX)
        return ((z + nz - d) % nz) * NC + core, s

    def from_above(j, core):
        d = (j + NX) // NX
        s = (j + NX) % NX
        s = jnp.where(j < 0, 2 * (j + half) + 1, jnp.where(j >= steps - half, s + half, s))
        return ((z + d) % nz) * NC + core, s

    up_copy(mine, 0, 0).start()
    low_copy(mine, 0, 0).start()
    side_copy(mine, 0, 0).start()
    x_copies = {}
    for d in order[1:]:
        to = (x + d) % NX
        x_copies[d] = remote(
            packkv.at[to],
            kv.at[mine, :, my_rows, :],
            xs_sem.at[d - 1],
            xr_sem.at[d - 1],
            dev(z, to, c),
        )
        x_copies[d].start()
    q_copies = []
    for d in order[1:]:
        to = (x + d) % NX
        copy = remote(
            packq.at[to],
            qrecv.at[my_rows, :],
            xs_sem.at[NX + d - 2],
            xr_sem.at[NX + d - 2],
            dev(z, to, c),
        )
        copy.start()
        q_copies.append(copy)
    for s, d in enumerate(order[1:], 1):
        x_copies[d].wait_recv()
        up_copy(mine, s, s).start()
        low_copy(mine, s, s).start()
        side_copy(mine, s, s).start()

    class Weight:
        def __init__(self, ref, n):
            self.ref = ref
            self.n = n

        def up(self, zz, k):
            block = self.ref.at[zz, x, c]
            at = self.n * mid + k - 1
            return remote(block, block, wus_sem.at[at], wur_sem.at[at], dev(z_up, x, c))

        def low(self, zz, k):
            block = self.ref.at[zz, x, c]
            at = self.n * mid + k - 1
            return remote(block, block, wls_sem.at[at], wlr_sem.at[at], dev(z_dn, x, c))

        def across(self, zz, d):
            block = self.ref.at[zz, x, c]
            at = (self.n * (NX - 1) + d - 1) * nz + zz
            return remote(block, block, wxs_sem.at[at], wxr_sem.at[at], dev(z, (x + d) % NX, c))

        def side(self, d):
            block = self.ref.at[:, (x + NX - d) % NX, c]
            at = self.n * NX + d
            return remote(block, block, wds_sem.at[at], wdr_sem.at[at], other)

        def begin(self):
            self.up(z, 1).start()
            self.low(z, 1).start()
            for d in order[1:]:
                self.across(z, d).start()

        def relay(self, k):
            below = (z + nz - k) % nz
            above = (z + k) % nz

            @pl.when((k < mid) | (c == 0))
            def _():
                self.up(below, k).wait_recv()

            @pl.when((k < mid) | (c == 1))
            def _():
                self.low(above, k).wait_recv()

            @pl.when((k < mid - 1) | ((k == mid - 1) & (c == 0)))
            def _():
                self.up(below, k + 1).start()

            @pl.when((k < mid - 1) | ((k == mid - 1) & (c == 1)))
            def _():
                self.low(above, k + 1).start()

            for d in order[1:]:
                self.across(below, d).start()

            @pl.when(k < mid)
            def _():
                for d in order[1:]:
                    self.across(above, d).start()

        def gather_side(self, d):
            if d:
                for zz in range(nz):
                    self.across(zz, d).wait_recv()
            self.side(d).start()

        def finish_side(self):
            for d in range(NX):
                self.side(d).wait_recv()

        def finish_sends(self):
            for k in range(1, mid):
                self.up(z, k).wait_send()
                self.low(z, k).wait_send()

            @pl.when(c == 0)
            def _():
                self.up(z, mid).wait_send()

            @pl.when(c == 1)
            def _():
                self.low(z, mid).wait_send()

            for d in range(1, NX):
                for zz in range(nz):
                    self.across(zz, d).wait_send()
            for d in range(NX):
                self.side(d).wait_send()

    w_out = Weight(wo, 0)
    w_down = Weight(wd, 1)
    loads[5].wait()
    w_out.begin()

    acc[...] = jnp.zeros_like(acc)
    tot[...] = jnp.zeros_like(tot)
    mx[...] = jnp.full(mx.shape, -3e38, F32)
    for copy in q_copies:
        copy.wait_recv()
    lane = lax.broadcasted_iota(jnp.int32, (rows, 128), 1) < 64
    queries = qrecv[...].astype(F32)
    qs[0:rows, :] = jnp.where(lane, queries, 0.0).astype(BF16)
    qs[rows : 2 * rows, :] = jnp.where(lane, 0.0, queries).astype(BF16)
    loads[6].wait()

    scale = 64 ** (-0.5) * math.log2(math.e)
    tile = min(256, 2 * rows)

    def attend(blocks):
        width = len(blocks) * tokens

        def body(r, carry):
            at = pl.ds(pl.multiple_of(r * tile, tile), tile)
            keys = jnp.concatenate([piece(slot, s)[0] for slot, s in blocks], axis=0)
            vals = jnp.concatenate([piece(slot, s)[1] for slot, s in blocks], axis=0)
            scores = dot_nt(qs[at, :], keys)
            old = mx[at, :]
            top = scores[:, 0:128]
            for lo in range(128, width, 128):
                top = jnp.maximum(top, scores[:, lo : lo + 128])
            new = jnp.maximum(old, jnp.max(top, axis=1, keepdims=True))
            factor = jnp.exp2((old - new) * scale)
            total = tot[at, :] * factor
            parts = []
            for lo in range(0, width, 128):
                part = jnp.exp2((scores[:, lo : lo + 128] - new) * scale)
                total = total + part
                parts.append(part.astype(BF16))
            mx[at, :] = new
            tot[at, :] = total
            acc[at, :] = acc[at, :] * factor + jnp.dot(
                jnp.concatenate(parts, axis=1), vals, preferred_element_type=F32
            )
            return carry

        lax.fori_loop(0, 2 * rows // tile, body, 0)

    attend([(mine, s) for s in range(NX)])

    def step(i, carry):
        below, below_s = from_below(i, c)
        above, above_s = from_above(i, c)
        up_copy(below, below_s, i).wait_recv()

        @pl.when(i < steps - NX)
        def _():
            up_copy(below, below_s, i + NX).start()

        low_copy(above, above_s, i).wait_recv()

        @pl.when((i < steps - NX - half) | ((i >= steps - NX) & (i < steps - half)))
        def _():
            to = jnp.where(i < steps - NX - half, i + NX, i + half)
            low_copy(above, above_s, to).start()

        side_copy(below, below_s, NX + i).start()
        side_copy(above, above_s, NX + steps + i).start()

        @pl.when((i % 2 == 1) & (i < 2 * mid))
        def _():
            w_out.relay((i + 1) // 2)

        @pl.when(i == DOWN_AT)
        def _():
            w_down.begin()

        @pl.when((i % 2 == 0) & (i > DOWN_AT) & (i <= DOWN_AT + 2 * mid))
        def _():
            w_down.relay((i - DOWN_AT) // 2)

        other_b, other_bs = from_below(i - half, 1 - c)
        other_a, other_as = from_above(i - half, 1 - c)
        b_index = jnp.where(i < half, 2 * i, NX + i - half)
        a_index = jnp.where(i < half, 2 * i + 1, NX + steps + i - half)
        side_copy(other_b, other_bs, b_index).wait_recv()
        side_copy(other_a, other_as, a_index).wait_recv()
        attend([(below, below_s), (above, above_s), (other_b, other_bs), (other_a, other_as)])
        return carry

    lax.fori_loop(0, steps, step, 0)
    w_out.gather_side(0)
    last = []
    for j in range(steps - half, steps):
        b = from_below(j, 1 - c)
        a = from_above(j, 1 - c)
        side_copy(*b, NX + j).wait_recv()
        side_copy(*a, NX + steps + j).wait_recv()
        last += [b, a]
    for d in order[1:]:
        w_out.gather_side(d)
    attend(last)

    weight = lam_ref[x]
    for j in range(NX):
        a, b = j * tokens, rows + j * tokens
        first = acc[a : a + tokens, :] / jnp.sum(tot[a : a + tokens, :], axis=1, keepdims=True)
        second = acc[b : b + tokens, :] / jnp.sum(tot[b : b + tokens, :], axis=1, keepdims=True)
        diff = first - weight * second
        normal = diff * lax.rsqrt(jnp.mean(diff * diff, axis=1, keepdims=True) + EPS)
        asend[j] = (normal * hgain_ref[...]).astype(BF16)

    my_cols = pl.ds(pl.multiple_of(x * 128, 128), 128)
    a_copies = []
    for d in order[1:]:
        to = (x + d) % NX
        copy = remote(
            asend.at[to],
            arecv.at[:, my_cols],
            as_sem.at[d - 1],
            ar_sem.at[d - 1],
            dev(z, to, c),
        )
        copy.start()
        a_copies.append(copy)
    arecv[:, my_cols] = asend[x]
    w_out.finish_side()
    for copy in a_copies:
        copy.wait()

    n_rows = res.shape[0]
    width = wo.shape[4]
    hidden_width = wd.shape[4]
    feature_rows = NX * NC * wo.shape[3]

    def exchange(send, recv, s_sem, r_sem):
        copies = []
        for d in range(1, n_tp):
            to = (tp + d) % n_tp
            copy = remote(send.at[to], recv.at[d - 1], s_sem.at[d - 1], r_sem.at[d - 1], (sp, to))
            copy.start()
            copies.append(copy)
        return copies

    def project(i, carry):
        at = pl.ds(pl.multiple_of(i * feature_rows, feature_rows), feature_rows)
        part = dot_nt(arecv[...], wo[i].reshape(feature_rows, width)).astype(BF16)
        for t in range(n_tp):
            psend[t, :, at] = part[t * n_rows : (t + 1) * n_rows, :]
        return carry

    lax.fori_loop(0, nz, project, 0)
    copies = exchange(psend, precv, ps_sem, pr_sem)
    loads[9].wait()
    total = psend[tp].astype(F32)
    for copy in copies:
        copy.wait()
    for d in range(n_tp - 1):
        total = total + precv[d].astype(F32)
    summed = (res[...].astype(F32) + total).astype(BF16)
    after[...] = summed
    stream = summed.astype(F32)
    normal = stream * lax.rsqrt(jnp.mean(stream * stream, axis=1, keepdims=True) + EPS)
    normed = (normal * ngain_ref[...]).astype(BF16)
    nsend[...] = normed
    my_part = pl.ds(pl.multiple_of(tp * n_rows, n_rows), n_rows)
    copies = []
    for d in range(1, n_tp):
        copy = remote(
            nsend,
            shard.at[my_part, :],
            ns_sem.at[d - 1],
            nr_sem.at[d - 1],
            (sp, (tp + d) % n_tp),
        )
        copy.start()
        copies.append(copy)
    shard[my_part, :] = normed
    w_down.gather_side(0)
    loads[7].wait()
    loads[8].wait()
    for copy in copies:
        copy.wait()
    lo = 0
    while lo < hidden_width:
        hi = min(lo + 256, hidden_width)
        gate = jnp.dot(shard[...], gv[:, lo:hi], preferred_element_type=F32)
        up = jnp.dot(shard[...], uv[:, lo:hi], preferred_element_type=F32)
        hid[:, lo:hi] = (gate / (1.0 + jnp.exp(-gate)) * up).astype(BF16)
        lo = hi
    for d in order[1:]:
        w_down.gather_side(d)
    w_down.finish_side()

    def down(i, carry):
        at = pl.ds(pl.multiple_of(i * feature_rows, feature_rows), feature_rows)
        part = dot_nt(hid[...], wd[i].reshape(feature_rows, hidden_width)).astype(BF16)
        for t in range(n_tp):
            dsend[t, :, at] = part[t * n_rows : (t + 1) * n_rows, :]
        return carry

    lax.fori_loop(0, nz, down, 0)
    copies = exchange(dsend, drecv, fs_sem, fr_sem)

    for d in range(1, NX):
        x_copies[d].wait_send()
    for copy in q_copies:
        copy.wait_send()
    for n in range(steps):
        up_copy(mine, 0, n).wait_send()
        low_copy(mine, 0, n).wait_send()
    for n in range(NX + 2 * steps):
        side_copy(mine, 0, n).wait_send()
    w_out.finish_sends()
    w_down.finish_sends()

    total = dsend[tp].astype(F32)
    for copy in copies:
        copy.wait()
    for d in range(n_tp - 1):
        total = total + drecv[d].astype(F32)
    out_ref[...] = (after[...].astype(F32) + total).astype(BF16)


def local(nz, n_tp, residual, q1, k1, q2, k2, v, lam, head_gain, out_w, norm_gain, gate, up, down):
    tokens = q1.shape[0]
    rows = NX * tokens
    n_rows, features = residual.shape
    hidden = gate.shape[1]
    steps = NX * (nz - 1) // 2
    mid = nz // 2
    vmem = pl.BlockSpec(memory_space=pltpu.VMEM)
    smem = pl.BlockSpec(memory_space=pltpu.SMEM)
    hbm = pl.BlockSpec(memory_space=pl.ANY)
    dma = pltpu.SemaphoreType.DMA

    def like(a):
        return pltpu.VMEM(a.shape, a.dtype)

    return pl.pallas_call(
        functools.partial(kernel, nz, n_tp),
        out_shape=jax.ShapeDtypeStruct((n_rows, features), BF16),
        in_specs=[hbm] * 6 + [smem, vmem, hbm, vmem, hbm, hbm, hbm],
        out_specs=vmem,
        scratch_shapes=[
            like(residual),
            like(q1),
            like(k1),
            like(q2),
            like(k2),
            like(v),
            like(gate),
            like(up),
            pltpu.VMEM((nz, NX, NC, *out_w.shape), BF16),
            pltpu.VMEM((nz, NX, NC, *down.shape), BF16),
            pltpu.VMEM((NX, tokens, 128), BF16),
            pltpu.VMEM((NX, 2, tokens, 128), BF16),
            pltpu.VMEM((rows, 128), BF16),
            pltpu.VMEM((2 * rows, 128), BF16),
            pltpu.VMEM((nz * NC, 2, rows, 128), BF16),
            pltpu.VMEM((2 * rows, 128), F32),
            pltpu.VMEM((2 * rows, 128), F32),
            pltpu.VMEM((2 * rows, 128), F32),
            pltpu.VMEM((NX, tokens, 128), BF16),
            pltpu.VMEM((tokens, NX * 128), BF16),
            pltpu.VMEM((n_tp, n_rows, features), BF16),
            pltpu.VMEM((n_tp - 1, n_rows, features), BF16),
            pltpu.VMEM((n_rows, features), BF16),
            pltpu.VMEM((n_rows, features), BF16),
            pltpu.VMEM((tokens, features), BF16),
            pltpu.VMEM((tokens, hidden), BF16),
            pltpu.VMEM((n_tp, n_rows, features), BF16),
            pltpu.VMEM((n_tp - 1, n_rows, features), BF16),
            dma((10,)),
            dma((2 * (NX - 1),)),
            dma((2 * (NX - 1),)),
            dma((steps,)),
            dma((steps,)),
            dma((steps,)),
            dma((steps,)),
            dma((NX + 2 * steps,)),
            dma((NX + 2 * steps,)),
            dma((NX - 1,)),
            dma((NX - 1,)),
            dma((2 * mid,)),
            dma((2 * mid,)),
            dma((2 * mid,)),
            dma((2 * mid,)),
            dma((2 * (NX - 1) * nz,)),
            dma((2 * (NX - 1) * nz,)),
            dma((2 * NX,)),
            dma((2 * NX,)),
            dma((n_tp - 1,)),
            dma((n_tp - 1,)),
            dma((n_tp - 1,)),
            dma((n_tp - 1,)),
            dma((n_tp - 1,)),
            dma((n_tp - 1,)),
        ],
        compiler_params=pltpu.CompilerParams(
            collective_id=0, has_side_effects=True, vmem_limit_bytes=62 * 2**20
        ),
        name="layer",
    )(
        residual,
        q1,
        k1,
        q2,
        k2,
        v,
        lam,
        head_gain.reshape(1, 128),
        out_w,
        norm_gain.reshape(1, features),
        gate,
        up,
        down,
    )


def solution(mesh):
    nz = mesh.shape["sp"] // (NX * NC)
    n_tp = mesh.shape["tp"]
    return jax.shard_map(
        functools.partial(local, nz, n_tp),
        mesh=mesh,
        in_specs=(
            P(("sp", "tp"), None),
            P("sp", "tp"),
            P("sp", "tp"),
            P("sp", "tp"),
            P("sp", "tp"),
            P("sp", "tp"),
            P("tp"),
            P(),
            P("sp", "tp"),
            P(),
            P(None, "tp"),
            P(None, "tp"),
            P("sp", "tp"),
        ),
        out_specs=P(("sp", "tp"), None),
        check_vma=False,
    )
```

```python
import functools
import math

import jax
import jax.numpy as jnp
from jax import lax
from jax.experimental import pallas as pl
from jax.experimental.pallas import tpu as pltpu
from jax.sharding import PartitionSpec as P

EPS = 1e-06
MESH = pl.DeviceIdType.MESH
NX = 4
NC = 2
DOWN_AT = 4
EARLY = 2
OUT_ON = 5
DOWN_ON = 10
DOWN_N = 2
PARTS = 4
F32 = jnp.float32
BF16 = jnp.bfloat16


def dot_nt(a, b):
    return lax.dot_general(a, b, (((1,), (1,)), ((), ())), preferred_element_type=F32)


def remote(src, dst, send, recv, device):
    return pltpu.make_async_remote_copy(
        src_ref=src,
        dst_ref=dst,
        send_sem=send,
        recv_sem=recv,
        device_id=device,
        device_id_type=MESH,
    )


def kernel(
    nz,
    n_tp,
    res_hbm,
    q1_hbm,
    k1_hbm,
    q2_hbm,
    k2_hbm,
    v_hbm,
    lam_ref,
    hgain_ref,
    outw_hbm,
    ngain_ref,
    gate_hbm,
    up_hbm,
    downw_hbm,
    out_ref,
    res,
    q1,
    k1,
    q2,
    k2,
    v,
    gv,
    uv,
    wo,
    wd,
    packq,
    packkv,
    qrecv,
    qs,
    kv,
    acc,
    mx,
    tot,
    asend,
    arecv,
    psend,
    precv,
    after,
    nsend,
    shard,
    gacc,
    uacc,
    hid,
    dsend,
    drecv,
    load_sem,
    xs_sem,
    xr_sem,
    us_sem,
    ur_sem,
    ls_sem,
    lr_sem,
    ds_sem,
    dr_sem,
    as_sem,
    ar_sem,
    wus_sem,
    wur_sem,
    wls_sem,
    wlr_sem,
    wxs_sem,
    wxr_sem,
    wds_sem,
    wdr_sem,
    ps_sem,
    pr_sem,
    ns_sem,
    nr_sem,
    fs_sem,
    fr_sem,
):
    sp = lax.axis_index("sp")
    tp = lax.axis_index("tp")
    z = sp // (NX * NC)
    x = (sp // NC) % NX
    c = sp % NC
    tokens = q1.shape[0]
    rows = NX * tokens
    steps = NX * (nz - 1) // 2
    mid = nz // 2
    half = NX // 2

    def dev(zz, xx, cc):
        return ((zz * NX + xx) * NC + cc, tp)

    z_up = (z + 1) % nz
    z_dn = (z + nz - 1) % nz
    other = dev(z, x, 1 - c)

    loads = []
    for n, (src, dst) in enumerate(
        (
            (k1_hbm, k1),
            (k2_hbm, k2),
            (v_hbm, v),
            (q1_hbm, q1),
            (q2_hbm, q2),
            (outw_hbm, wo.at[z, x, c]),
            (downw_hbm, wd.at[z, x, c]),
            (gate_hbm, gv),
            (up_hbm, uv),
            (res_hbm, res),
        )
    ):
        load = pltpu.make_async_copy(src, dst, load_sem.at[n])
        load.start()
        loads.append(load)

    peers = [dev(z, (x + d) % NX, c) for d in range(1, NX)]
    peers += [dev(z_up, x, c), dev(z_dn, x, c), other]
    peers += [(sp, (tp + d) % n_tp) for d in range(1, n_tp)]
    barrier = pltpu.get_barrier_semaphore()
    for p in peers:
        pl.semaphore_signal(barrier, inc=1, device_id=p, device_id_type=MESH)

    low = lax.broadcasted_iota(jnp.int32, (tokens, 128), 1) < 64

    def joined(first, second, j):
        a = first[:, 128 * (j // 2) : 128 * (j // 2) + 128].astype(F32)
        b = second[:, 128 * (j // 2) : 128 * (j // 2) + 128].astype(F32)
        if j % 2 == 0:
            b = pltpu.roll(b, 64, 1)
        else:
            a = pltpu.roll(a, 64, 1)
        return jnp.where(low, a, b).astype(BF16)

    mine = z * NC + c
    my_rows = pl.ds(pl.multiple_of(x * tokens, tokens), tokens)
    for load in loads[:3]:
        load.wait()
    for j in range(NX):
        packkv[j, 0] = joined(k1, k2, j)
        packkv[j, 1] = v[:, 128 * j : 128 * j + 128]
    kv[mine, :, my_rows, :] = packkv[x]
    for load in loads[3:5]:
        load.wait()
    for j in range(NX):
        packq[j] = joined(q1, q2, j)
    qrecv[my_rows, :] = packq[x]
    pl.semaphore_wait(barrier, len(peers))

    order = [0, 1, NX - 1] + list(range(2, NX - 1))

    def source(s):
        back = s
        for n, d in enumerate(order):
            back = jnp.where(s == n, d, back)
        return (x + NX - back) % NX

    def piece(slot, s):
        at = pl.multiple_of(source(s) * tokens, tokens)
        return kv.at[slot, :, pl.ds(at, tokens), :]

    def up_copy(slot, s, index):
        part = piece(slot, s)
        return remote(part, part, us_sem.at[index], ur_sem.at[index], dev(z_up, x, c))

    def low_copy(slot, s, index):
        part = piece(slot, s)
        return remote(part, part, ls_sem.at[index], lr_sem.at[index], dev(z_dn, x, c))

    def side_copy(slot, s, index):
        part = piece(slot, s)
        return remote(part, part, ds_sem.at[index], dr_sem.at[index], other)

    def from_below(j, core):
        d = (j + NX) // NX
        s = jnp.where(j < 0, 2 * (j + half), (j + NX) % NX)
        return ((z + nz - d) % nz) * NC + core, s

    def from_above(j, core):
        d = (j + NX) // NX
        s = (j + NX) % NX
        s = jnp.where(j < 0, 2 * (j + half) + 1, jnp.where(j >= steps - half, s + half, s))
        return ((z + d) % nz) * NC + core, s

    up_copy(mine, 0, 0).start()
    low_copy(mine, 0, 0).start()
    side_copy(mine, 0, 0).start()
    x_copies = {}
    for d in order[1:]:
        to = (x + d) % NX
        x_copies[d] = remote(
            packkv.at[to],
            kv.at[mine, :, my_rows, :],
            xs_sem.at[d - 1],
            xr_sem.at[d - 1],
            dev(z, to, c),
        )
        x_copies[d].start()
    q_copies = []
    for d in order[1:]:
        to = (x + d) % NX
        copy = remote(
            packq.at[to],
            qrecv.at[my_rows, :],
            xs_sem.at[NX + d - 2],
            xr_sem.at[NX + d - 2],
            dev(z, to, c),
        )
        copy.start()
        q_copies.append(copy)
    for s, d in enumerate(order[1:], 1):
        x_copies[d].wait_recv()
        up_copy(mine, s, s).start()
        low_copy(mine, s, s).start()
        side_copy(mine, s, s).start()

    class Weight:
        def __init__(self, ref, n, early):
            self.ref = ref
            self.n = n
            self.early = early

        def up(self, zz, k):
            block = self.ref.at[zz, x, c]
            at = self.n * mid + k - 1
            return remote(block, block, wus_sem.at[at], wur_sem.at[at], dev(z_up, x, c))

        def low(self, zz, k):
            block = self.ref.at[zz, x, c]
            at = self.n * mid + k - 1
            return remote(block, block, wls_sem.at[at], wlr_sem.at[at], dev(z_dn, x, c))

        def across(self, zz, d):
            block = self.ref.at[zz, x, c]
            at = (self.n * (NX - 1) + d - 1) * nz + zz
            return remote(block, block, wxs_sem.at[at], wxr_sem.at[at], dev(z, (x + d) % NX, c))

        def side(self, d):
            block = self.ref.at[:, (x + NX - d) % NX, c]
            at = self.n * NX + d
            return remote(block, block, wds_sem.at[at], wdr_sem.at[at], other)

        def begin(self):
            self.up(z, 1).start()
            self.low(z, 1).start()
            self.across(z, 1).start()
            self.across(z, NX - 1).start()

        def relay(self, k):
            below = (z + nz - k) % nz
            above = (z + k) % nz

            @pl.when((k < mid) | (c == 0))
            def _():
                self.up(below, k).wait_recv()

            @pl.when((k < mid) | (c == 1))
            def _():
                self.low(above, k).wait_recv()

            @pl.when((k < mid - 1) | ((k == mid - 1) & (c == 0)))
            def _():
                self.up(below, k + 1).start()

            @pl.when((k < mid - 1) | ((k == mid - 1) & (c == 1)))
            def _():
                self.low(above, k + 1).start()

            @pl.when(k <= self.early)
            def _():
                for d in (1, NX - 1):
                    self.across(below, d).start()

            @pl.when((k <= self.early) & (k < mid))
            def _():
                for d in (1, NX - 1):
                    self.across(above, d).start()

        def late(self):
            for k in range(self.early + 1, mid + 1):
                for zz in ((z + nz - k) % nz, (z + k) % nz)[: 1 + (k < mid)]:
                    for d in (1, NX - 1):
                        self.across(zz, d).start()

        def second(self, zz, d):
            block = self.ref.at[zz, (x + NX - d) % NX, c]
            at = (self.n * (NX - 1) + 1) * nz + zz
            return remote(block, block, wxs_sem.at[at], wxr_sem.at[at], dev(z, (x + d) % NX, c))

        def onward(self, k):
            below = (z + nz - k) % nz
            above = (z + k) % nz
            both = (k > 0) & (k < mid)

            @pl.when(both | (c == 0))
            def _():
                self.across(below, 1).wait_recv()
                self.second(below, 1).start()

            @pl.when(both | (c == 1))
            def _():
                self.across(above, NX - 1).wait_recv()
                self.second(above, NX - 1).start()

        def gather_side(self, d):
            if d == 1 or d == NX - 1:
                for k in range(1, mid):
                    zz = (z + k) % nz if d == 1 else (z + nz - k) % nz
                    self.across(zz, d).wait_recv()

                @pl.when(c == (1 if d == 1 else 0))
                def _():
                    self.across(z, d).wait_recv()
                    self.across((z + mid) % nz, d).wait_recv()

            elif d:
                for zz in range(nz):
                    self.across(zz, d).wait_recv()
            self.side(d).start()

        def finish_side(self):
            for d in range(NX):
                self.side(d).wait_recv()

        def finish_sends(self):
            for k in range(1, mid):
                self.up(z, k).wait_send()
                self.low(z, k).wait_send()

            @pl.when(c == 0)
            def _():
                self.up(z, mid).wait_send()

            @pl.when(c == 1)
            def _():
                self.low(z, mid).wait_send()

            for d in range(1, NX):
                for zz in range(nz):
                    self.across(zz, d).wait_send()
            for d in range(NX):
                self.side(d).wait_send()

    w_out = Weight(wo, 0, mid)
    w_down = Weight(wd, 1, EARLY)
    loads[5].wait()
    w_out.begin()

    acc[...] = jnp.zeros_like(acc)
    tot[...] = jnp.zeros_like(tot)
    mx[...] = jnp.full(mx.shape, -3e38, F32)
    for copy in q_copies:
        copy.wait_recv()
    lane = lax.broadcasted_iota(jnp.int32, (rows, 128), 1) < 64
    queries = qrecv[...].astype(F32)
    qs[0:rows, :] = jnp.where(lane, queries, 0.0).astype(BF16)
    qs[rows : 2 * rows, :] = jnp.where(lane, 0.0, queries).astype(BF16)
    loads[6].wait()

    scale = 64 ** (-0.5) * math.log2(math.e)
    tile = rows

    def attend(blocks):
        width = len(blocks) * tokens
        keys = jnp.concatenate([piece(slot, s)[0] for slot, s in blocks], axis=0)
        vals = jnp.concatenate([piece(slot, s)[1] for slot, s in blocks], axis=0)
        halves = [pl.ds(n * tile, tile) for n in range(2)]
        for at, scores in [(at, dot_nt(qs[at, :], keys)) for at in halves]:
            old = mx[at, :]
            top = scores[:, 0:128]
            for lo in range(128, width, 128):
                top = jnp.maximum(top, scores[:, lo : lo + 128])
            new = jnp.maximum(old, jnp.max(top, axis=1, keepdims=True))
            factor = jnp.exp2((old - new) * scale)
            total = tot[at, :] * factor
            parts = []
            for lo in range(0, width, 128):
                part = jnp.exp2((scores[:, lo : lo + 128] - new) * scale)
                total = total + part
                parts.append(part.astype(BF16))
            mx[at, :] = new
            tot[at, :] = total
            acc[at, :] = acc[at, :] * factor + jnp.dot(
                jnp.concatenate(parts, axis=1), vals, preferred_element_type=F32
            )

    attend([(mine, s) for s in range(NX)])

    def step(i, carry):
        below, below_s = from_below(i, c)
        above, above_s = from_above(i, c)
        up_copy(below, below_s, i).wait_recv()

        @pl.when(i < steps - NX)
        def _():
            up_copy(below, below_s, i + NX).start()

        low_copy(above, above_s, i).wait_recv()

        @pl.when((i < steps - NX - half) | ((i >= steps - NX) & (i < steps - half)))
        def _():
            to = jnp.where(i < steps - NX - half, i + NX, i + half)
            low_copy(above, above_s, to).start()

        side_copy(below, below_s, NX + i).start()
        side_copy(above, above_s, NX + steps + i).start()

        @pl.when((i % 2 == 1) & (i < 2 * mid))
        def _():
            w_out.relay((i + 1) // 2)

        @pl.when((i % 2 == 1) & (i >= OUT_ON) & (i <= OUT_ON + 2 * mid))
        def _():
            w_out.onward((i - OUT_ON) // 2)

        @pl.when((i % 2 == 0) & (i >= DOWN_ON) & (i < DOWN_ON + 2 * DOWN_N))
        def _():
            w_down.onward((i - DOWN_ON) // 2)

        @pl.when(i == DOWN_AT)
        def _():
            w_down.begin()

        @pl.when((i % 2 == 0) & (i > DOWN_AT) & (i <= DOWN_AT + 2 * mid))
        def _():
            w_down.relay((i - DOWN_AT) // 2)

        other_b, other_bs = from_below(i - half, 1 - c)
        other_a, other_as = from_above(i - half, 1 - c)
        b_index = jnp.where(i < half, 2 * i, NX + i - half)
        a_index = jnp.where(i < half, 2 * i + 1, NX + steps + i - half)
        side_copy(other_b, other_bs, b_index).wait_recv()
        side_copy(other_a, other_as, a_index).wait_recv()
        attend([(below, below_s), (above, above_s), (other_b, other_bs), (other_a, other_as)])
        return carry

    lax.fori_loop(0, steps, step, 0)
    w_out.gather_side(0)
    last = []
    for j in range(steps - half, steps):
        b = from_below(j, 1 - c)
        a = from_above(j, 1 - c)
        side_copy(*b, NX + j).wait_recv()
        side_copy(*a, NX + steps + j).wait_recv()
        last += [b, a]
    for d in order[1:]:
        w_out.gather_side(d)
    attend(last)

    weight = lam_ref[x]
    for j in range(NX):
        a, b = j * tokens, rows + j * tokens
        first = acc[a : a + tokens, :] / jnp.sum(tot[a : a + tokens, :], axis=1, keepdims=True)
        second = acc[b : b + tokens, :] / jnp.sum(tot[b : b + tokens, :], axis=1, keepdims=True)
        diff = first - weight * second
        normal = diff * lax.rsqrt(jnp.mean(diff * diff, axis=1, keepdims=True) + EPS)
        asend[j] = (normal * hgain_ref[...]).astype(BF16)

    my_cols = pl.ds(pl.multiple_of(x * 128, 128), 128)
    a_copies = []
    for d in order[1:]:
        to = (x + d) % NX
        copy = remote(
            asend.at[to],
            arecv.at[:, my_cols],
            as_sem.at[d - 1],
            ar_sem.at[d - 1],
            dev(z, to, c),
        )
        copy.start()
        a_copies.append(copy)
    arecv[:, my_cols] = asend[x]
    w_down.late()
    w_out.finish_side()
    for copy in a_copies:
        copy.wait()

    n_rows = res.shape[0]
    width = wo.shape[4]
    hidden_width = wd.shape[4]
    feature_rows = NX * NC * wo.shape[3]

    cols = wo.shape[0] * feature_rows // PARTS
    per_part = nz // PARTS

    def project(rows_ref, weights, k_width, send, recv, s_sem, r_sem):
        copies = []
        for p in range(PARTS):
            at = pl.ds(p * cols, cols)
            w = weights[p * per_part : (p + 1) * per_part].reshape(cols, k_width)
            part = dot_nt(rows_ref[...], w).astype(BF16)
            for t in range(n_tp):
                send[t, :, at] = part[t * n_rows : (t + 1) * n_rows, :]
            for d in range(1, n_tp):
                to = (tp + d) % n_tp
                n = p * (n_tp - 1) + d - 1
                copy = remote(
                    send.at[to, :, at],
                    recv.at[d - 1, :, at],
                    s_sem.at[n],
                    r_sem.at[n],
                    (sp, to),
                )
                copy.start()
                copies.append(copy)
        return copies

    copies = project(arecv, wo, width, psend, precv, ps_sem, pr_sem)
    for k in range(DOWN_N, EARLY + 1):
        w_down.onward(k)
    loads[9].wait()
    total = psend[tp].astype(F32)
    for copy in copies:
        copy.wait()
    for d in range(n_tp - 1):
        total = total + precv[d].astype(F32)
    summed = (res[...].astype(F32) + total).astype(BF16)
    after[...] = summed
    stream = summed.astype(F32)
    normal = stream * lax.rsqrt(jnp.mean(stream * stream, axis=1, keepdims=True) + EPS)
    normed = (normal * ngain_ref[...]).astype(BF16)
    nsend[...] = normed
    my_part = pl.ds(pl.multiple_of(tp * n_rows, n_rows), n_rows)
    copies = []
    middle = nsend.shape[1] // 2
    sides = (pl.ds(0, middle), pl.ds(middle, middle))
    for n, side in enumerate(sides):
        for d in range(1, n_tp):
            copy = remote(
                nsend.at[:, side],
                shard.at[my_part, side],
                ns_sem.at[n * (n_tp - 1) + d - 1],
                nr_sem.at[n * (n_tp - 1) + d - 1],
                (sp, (tp + d) % n_tp),
            )
            copy.start()
            copies.append(copy)
    shard[my_part, :] = normed
    w_down.gather_side(0)
    for k in range(EARLY + 1, mid + 1):
        w_down.onward(k)
    loads[7].wait()
    loads[8].wait()
    tiles = [(lo, min(lo + 256, hidden_width)) for lo in range(0, hidden_width, 256)]
    for copy in copies[: n_tp - 1]:
        copy.wait()
    for lo, hi in tiles:
        left = shard[:, 0:middle]
        gacc[:, lo:hi] = jnp.dot(left, gv[0:middle, lo:hi], preferred_element_type=F32)
        uacc[:, lo:hi] = jnp.dot(left, uv[0:middle, lo:hi], preferred_element_type=F32)
    for copy in copies[n_tp - 1 :]:
        copy.wait()
    for lo, hi in tiles:
        left = shard[:, middle:]
        gate = gacc[:, lo:hi] + jnp.dot(left, gv[middle:, lo:hi], preferred_element_type=F32)
        up = uacc[:, lo:hi] + jnp.dot(left, uv[middle:, lo:hi], preferred_element_type=F32)
        hid[:, lo:hi] = (gate / (1.0 + jnp.exp(-gate)) * up).astype(BF16)
    for d in order[1:]:
        w_down.gather_side(d)
    w_down.finish_side()

    copies = project(hid, wd, hidden_width, dsend, drecv, fs_sem, fr_sem)

    for d in range(1, NX):
        x_copies[d].wait_send()
    for copy in q_copies:
        copy.wait_send()
    for n in range(steps):
        up_copy(mine, 0, n).wait_send()
        low_copy(mine, 0, n).wait_send()
    for n in range(NX + 2 * steps):
        side_copy(mine, 0, n).wait_send()
    w_out.finish_sends()
    w_down.finish_sends()

    total = dsend[tp].astype(F32)
    for copy in copies:
        copy.wait()
    for d in range(n_tp - 1):
        total = total + drecv[d].astype(F32)
    out_ref[...] = (after[...].astype(F32) + total).astype(BF16)


def local(nz, n_tp, residual, q1, k1, q2, k2, v, lam, head_gain, out_w, norm_gain, gate, up, down):
    tokens = q1.shape[0]
    rows = NX * tokens
    n_rows, features = residual.shape
    hidden = gate.shape[1]
    steps = NX * (nz - 1) // 2
    mid = nz // 2
    vmem = pl.BlockSpec(memory_space=pltpu.VMEM)
    smem = pl.BlockSpec(memory_space=pltpu.SMEM)
    hbm = pl.BlockSpec(memory_space=pl.ANY)
    dma = pltpu.SemaphoreType.DMA

    def like(a):
        return pltpu.VMEM(a.shape, a.dtype)

    return pl.pallas_call(
        functools.partial(kernel, nz, n_tp),
        out_shape=jax.ShapeDtypeStruct((n_rows, features), BF16),
        in_specs=[hbm] * 6 + [smem, vmem, hbm, vmem, hbm, hbm, hbm],
        out_specs=vmem,
        scratch_shapes=[
            like(residual),
            like(q1),
            like(k1),
            like(q2),
            like(k2),
            like(v),
            like(gate),
            like(up),
            pltpu.VMEM((nz, NX, NC, *out_w.shape), BF16),
            pltpu.VMEM((nz, NX, NC, *down.shape), BF16),
            pltpu.VMEM((NX, tokens, 128), BF16),
            pltpu.VMEM((NX, 2, tokens, 128), BF16),
            pltpu.VMEM((rows, 128), BF16),
            pltpu.VMEM((2 * rows, 128), BF16),
            pltpu.VMEM((nz * NC, 2, rows, 128), BF16),
            pltpu.VMEM((2 * rows, 128), F32),
            pltpu.VMEM((2 * rows, 128), F32),
            pltpu.VMEM((2 * rows, 128), F32),
            pltpu.VMEM((NX, tokens, 128), BF16),
            pltpu.VMEM((tokens, NX * 128), BF16),
            pltpu.VMEM((n_tp, n_rows, features), BF16),
            pltpu.VMEM((n_tp - 1, n_rows, features), BF16),
            pltpu.VMEM((n_rows, features), BF16),
            pltpu.VMEM((n_rows, features), BF16),
            pltpu.VMEM((tokens, features), BF16),
            pltpu.VMEM((tokens, hidden), F32),
            pltpu.VMEM((tokens, hidden), F32),
            pltpu.VMEM((tokens, hidden), BF16),
            pltpu.VMEM((n_tp, n_rows, features), BF16),
            pltpu.VMEM((n_tp - 1, n_rows, features), BF16),
            dma((10,)),
            dma((2 * (NX - 1),)),
            dma((2 * (NX - 1),)),
            dma((steps,)),
            dma((steps,)),
            dma((steps,)),
            dma((steps,)),
            dma((NX + 2 * steps,)),
            dma((NX + 2 * steps,)),
            dma((NX - 1,)),
            dma((NX - 1,)),
            dma((2 * mid,)),
            dma((2 * mid,)),
            dma((2 * mid,)),
            dma((2 * mid,)),
            dma((2 * (NX - 1) * nz,)),
            dma((2 * (NX - 1) * nz,)),
            dma((2 * NX,)),
            dma((2 * NX,)),
            dma((PARTS * (n_tp - 1),)),
            dma((PARTS * (n_tp - 1),)),
            dma((2 * (n_tp - 1),)),
            dma((2 * (n_tp - 1),)),
            dma((PARTS * (n_tp - 1),)),
            dma((PARTS * (n_tp - 1),)),
        ],
        compiler_params=pltpu.CompilerParams(
            collective_id=0, has_side_effects=True, vmem_limit_bytes=62 * 2**20
        ),
        name="layer",
    )(
        residual,
        q1,
        k1,
        q2,
        k2,
        v,
        lam,
        head_gain.reshape(1, 128),
        out_w,
        norm_gain.reshape(1, features),
        gate,
        up,
        down,
    )


def solution(mesh):
    nz = mesh.shape["sp"] // (NX * NC)
    n_tp = mesh.shape["tp"]
    return jax.shard_map(
        functools.partial(local, nz, n_tp),
        mesh=mesh,
        in_specs=(
            P(("sp", "tp"), None),
            P("sp", "tp"),
            P("sp", "tp"),
            P("sp", "tp"),
            P("sp", "tp"),
            P("sp", "tp"),
            P("tp"),
            P(),
            P("sp", "tp"),
            P(),
            P(None, "tp"),
            P(None, "tp"),
            P("sp", "tp"),
        ),
        out_specs=P(("sp", "tp"), None),
        check_vma=False,
    )
```

```python
import functools
import math

import jax
import jax.numpy as jnp
from jax import lax
from jax.experimental import pallas as pl
from jax.experimental.pallas import tpu as pltpu
from jax.sharding import PartitionSpec as P

EPS = 1e-06
MESH = pl.DeviceIdType.MESH
NX = 4
NC = 2
DOWN_AT = 6
OUT_ON = 5
PARTS = 4
F32 = jnp.float32
BF16 = jnp.bfloat16


def dot_nt(a, b):
    return lax.dot_general(a, b, (((1,), (1,)), ((), ())), preferred_element_type=F32)


def remote(src, dst, send, recv, device):
    return pltpu.make_async_remote_copy(
        src_ref=src,
        dst_ref=dst,
        send_sem=send,
        recv_sem=recv,
        device_id=device,
        device_id_type=MESH,
    )


def kernel(
    nz,
    n_tp,
    res_hbm,
    q1_hbm,
    k1_hbm,
    q2_hbm,
    k2_hbm,
    v_hbm,
    lam_ref,
    hgain_ref,
    outw_hbm,
    ngain_ref,
    gate_hbm,
    up_hbm,
    downw_hbm,
    out_ref,
    res,
    q1,
    k1,
    q2,
    k2,
    v,
    gv,
    uv,
    wo,
    wd,
    packq,
    packkv,
    qrecv,
    qs,
    kv,
    acc,
    mx,
    tot,
    asend,
    arecv,
    psend,
    precv,
    after,
    nsend,
    shard,
    gacc,
    uacc,
    hid,
    dsend,
    drecv,
    load_sem,
    xs_sem,
    xr_sem,
    us_sem,
    ur_sem,
    ls_sem,
    lr_sem,
    ds_sem,
    dr_sem,
    as_sem,
    ar_sem,
    wus_sem,
    wur_sem,
    wls_sem,
    wlr_sem,
    wxs_sem,
    wxr_sem,
    wds_sem,
    wdr_sem,
    ps_sem,
    pr_sem,
    ns_sem,
    nr_sem,
    fs_sem,
    fr_sem,
):
    sp = lax.axis_index("sp")
    tp = lax.axis_index("tp")
    z = sp // (NX * NC)
    x = (sp // NC) % NX
    c = sp % NC
    tokens = q1.shape[0]
    rows = NX * tokens
    steps = NX * (nz - 1) // 2
    mid = nz // 2
    half = NX // 2

    def dev(zz, xx, cc):
        return ((zz * NX + xx) * NC + cc, tp)

    z_up = (z + 1) % nz
    z_dn = (z + nz - 1) % nz
    other = dev(z, x, 1 - c)

    loads = []
    for n, (src, dst) in enumerate(
        (
            (k1_hbm, k1),
            (k2_hbm, k2),
            (v_hbm, v),
            (q1_hbm, q1),
            (q2_hbm, q2),
            (outw_hbm, wo.at[z, x, c]),
            (downw_hbm, wd.at[z, x, c]),
            (gate_hbm, gv),
            (up_hbm, uv),
            (res_hbm, res),
        )
    ):
        load = pltpu.make_async_copy(src, dst, load_sem.at[n])
        load.start()
        loads.append(load)

    peers = [dev(z, (x + d) % NX, c) for d in range(1, NX)]
    peers += [dev(z_up, x, c), dev(z_dn, x, c), other]
    peers += [(sp, (tp + d) % n_tp) for d in range(1, n_tp)]
    barrier = pltpu.get_barrier_semaphore()
    for p in peers:
        pl.semaphore_signal(barrier, inc=1, device_id=p, device_id_type=MESH)

    low = lax.broadcasted_iota(jnp.int32, (tokens, 128), 1) < 64

    def joined(first, second, j):
        a = first[:, 128 * (j // 2) : 128 * (j // 2) + 128].astype(F32)
        b = second[:, 128 * (j // 2) : 128 * (j // 2) + 128].astype(F32)
        if j % 2 == 0:
            b = pltpu.roll(b, 64, 1)
        else:
            a = pltpu.roll(a, 64, 1)
        return jnp.where(low, a, b).astype(BF16)

    mine = z * NC + c
    my_rows = pl.ds(pl.multiple_of(x * tokens, tokens), tokens)
    for load in loads[:3]:
        load.wait()
    for j in range(NX):
        packkv[j, 0] = joined(k1, k2, j)
        packkv[j, 1] = v[:, 128 * j : 128 * j + 128]
    kv[mine, :, my_rows, :] = packkv[x]
    for load in loads[3:5]:
        load.wait()
    for j in range(NX):
        packq[j] = joined(q1, q2, j)
    qrecv[my_rows, :] = packq[x]
    pl.semaphore_wait(barrier, len(peers))

    order = [0, 1, NX - 1] + list(range(2, NX - 1))

    def source(s):
        back = s
        for n, d in enumerate(order):
            back = jnp.where(s == n, d, back)
        return (x + NX - back) % NX

    def piece(slot, s):
        at = pl.multiple_of(source(s) * tokens, tokens)
        return kv.at[slot, :, pl.ds(at, tokens), :]

    def up_copy(slot, s, index):
        part = piece(slot, s)
        return remote(part, part, us_sem.at[index], ur_sem.at[index], dev(z_up, x, c))

    def low_copy(slot, s, index):
        part = piece(slot, s)
        return remote(part, part, ls_sem.at[index], lr_sem.at[index], dev(z_dn, x, c))

    def side_copy(slot, s, index):
        part = piece(slot, s)
        return remote(part, part, ds_sem.at[index], dr_sem.at[index], other)

    def from_below(j, core):
        d = (j + NX) // NX
        s = jnp.where(j < 0, 2 * (j + half), (j + NX) % NX)
        return ((z + nz - d) % nz) * NC + core, s

    def from_above(j, core):
        d = (j + NX) // NX
        s = (j + NX) % NX
        s = jnp.where(j < 0, 2 * (j + half) + 1, jnp.where(j >= steps - half, s + half, s))
        return ((z + d) % nz) * NC + core, s

    class Weight:
        def __init__(self, ref, n):
            self.ref = ref
            self.n = n

        def up(self, zz, k):
            block = self.ref.at[zz, x, c]
            at = self.n * mid + k - 1
            return remote(block, block, wus_sem.at[at], wur_sem.at[at], dev(z_up, x, c))

        def low(self, zz, k):
            block = self.ref.at[zz, x, c]
            at = self.n * mid + k - 1
            return remote(block, block, wls_sem.at[at], wlr_sem.at[at], dev(z_dn, x, c))

        def across(self, zz, d):
            block = self.ref.at[zz, x, c]
            at = (self.n * (NX - 1) + d - 1) * nz + zz
            return remote(block, block, wxs_sem.at[at], wxr_sem.at[at], dev(z, (x + d) % NX, c))

        def side(self, d):
            block = self.ref.at[:, (x + NX - d) % NX, c]
            at = self.n * NX + d
            return remote(block, block, wds_sem.at[at], wdr_sem.at[at], other)

        def begin(self):
            self.up(z, 1).start()
            self.low(z, 1).start()

        def begin_across(self):
            self.across(z, 1).start()
            self.across(z, NX - 1).start()

        def relay(self, k):
            below = (z + nz - k) % nz
            above = (z + k) % nz

            @pl.when((k < mid) | (c == 0))
            def _():
                self.up(below, k).wait_recv()

            @pl.when((k < mid) | (c == 1))
            def _():
                self.low(above, k).wait_recv()

            @pl.when((k < mid - 1) | ((k == mid - 1) & (c == 0)))
            def _():
                self.up(below, k + 1).start()

            @pl.when((k < mid - 1) | ((k == mid - 1) & (c == 1)))
            def _():
                self.low(above, k + 1).start()

        def spread(self, k):
            below = (z + nz - k) % nz
            above = (z + k) % nz
            for d in (1, NX - 1):
                self.across(below, d).start()

            @pl.when(k < mid)
            def _():
                for d in (1, NX - 1):
                    self.across(above, d).start()

        def second(self, zz, d):
            block = self.ref.at[zz, (x + NX - d) % NX, c]
            at = (self.n * (NX - 1) + 1) * nz + zz
            return remote(block, block, wxs_sem.at[at], wxr_sem.at[at], dev(z, (x + d) % NX, c))

        def onward(self, k):
            below = (z + nz - k) % nz
            above = (z + k) % nz
            both = (k > 0) & (k < mid)

            @pl.when(both | (c == 0))
            def _():
                self.across(below, 1).wait_recv()
                self.second(below, 1).start()

            @pl.when(both | (c == 1))
            def _():
                self.across(above, NX - 1).wait_recv()
                self.second(above, NX - 1).start()

        def gather_side(self, d):
            if d == 1 or d == NX - 1:
                for k in range(1, mid):
                    zz = (z + k) % nz if d == 1 else (z + nz - k) % nz
                    self.across(zz, d).wait_recv()

                @pl.when(c == (1 if d == 1 else 0))
                def _():
                    self.across(z, d).wait_recv()
                    self.across((z + mid) % nz, d).wait_recv()

            elif d:
                for zz in range(nz):
                    self.across(zz, d).wait_recv()
            self.side(d).start()

        def finish_side(self):
            for d in range(NX):
                self.side(d).wait_recv()

        def finish_sends(self):
            for k in range(1, mid):
                self.up(z, k).wait_send()
                self.low(z, k).wait_send()

            @pl.when(c == 0)
            def _():
                self.up(z, mid).wait_send()

            @pl.when(c == 1)
            def _():
                self.low(z, mid).wait_send()

            for d in range(1, NX):
                for zz in range(nz):
                    self.across(zz, d).wait_send()
            for d in range(NX):
                self.side(d).wait_send()

    w_out = Weight(wo, 0)
    w_down = Weight(wd, 1)
    up_copy(mine, 0, 0).start()
    low_copy(mine, 0, 0).start()
    side_copy(mine, 0, 0).start()
    x_copies = {}
    for d in order[1:]:
        to = (x + d) % NX
        x_copies[d] = remote(
            packkv.at[to],
            kv.at[mine, :, my_rows, :],
            xs_sem.at[d - 1],
            xr_sem.at[d - 1],
            dev(z, to, c),
        )
        x_copies[d].start()
    q_copies = []
    for d in order[1:]:
        to = (x + d) % NX
        copy = remote(
            packq.at[to],
            qrecv.at[my_rows, :],
            xs_sem.at[NX + d - 2],
            xr_sem.at[NX + d - 2],
            dev(z, to, c),
        )
        copy.start()
        q_copies.append(copy)
    for s, d in enumerate(order[1:], 1):
        x_copies[d].wait_recv()
        up_copy(mine, s, s).start()
        low_copy(mine, s, s).start()
        side_copy(mine, s, s).start()

    loads[5].wait()
    w_out.begin()
    w_out.begin_across()
    acc[...] = jnp.zeros_like(acc)
    tot[...] = jnp.zeros_like(tot)
    mx[...] = jnp.full(mx.shape, -3e38, F32)
    for copy in q_copies:
        copy.wait_recv()
    lane = lax.broadcasted_iota(jnp.int32, (rows, 128), 1) < 64
    queries = qrecv[...].astype(F32)
    qs[0:rows, :] = jnp.where(lane, queries, 0.0).astype(BF16)
    qs[rows : 2 * rows, :] = jnp.where(lane, 0.0, queries).astype(BF16)
    loads[6].wait()

    scale = 64 ** (-0.5) * math.log2(math.e)
    tile = rows

    def attend(blocks):
        width = len(blocks) * tokens
        keys = jnp.concatenate([piece(slot, s)[0] for slot, s in blocks], axis=0)
        vals = jnp.concatenate([piece(slot, s)[1] for slot, s in blocks], axis=0)
        halves = [pl.ds(n * tile, tile) for n in range(2)]
        for at, scores in [(at, dot_nt(qs[at, :], keys)) for at in halves]:
            old = mx[at, :]
            top = scores[:, 0:128]
            for lo in range(128, width, 128):
                top = jnp.maximum(top, scores[:, lo : lo + 128])
            new = jnp.maximum(old, jnp.max(top, axis=1, keepdims=True))
            factor = jnp.exp2((old - new) * scale)
            total = tot[at, :] * factor
            parts = []
            for lo in range(0, width, 128):
                part = jnp.exp2((scores[:, lo : lo + 128] - new) * scale)
                total = total + part
                parts.append(part.astype(BF16))
            mx[at, :] = new
            tot[at, :] = total
            acc[at, :] = acc[at, :] * factor + jnp.dot(
                jnp.concatenate(parts, axis=1), vals, preferred_element_type=F32
            )

    attend([(mine, s) for s in range(NX)])

    def step(i, carry):
        below, below_s = from_below(i, c)
        above, above_s = from_above(i, c)
        up_copy(below, below_s, i).wait_recv()

        @pl.when(i == DOWN_AT)
        def _():
            w_down.begin()

        @pl.when((i > DOWN_AT) & ((i - DOWN_AT) % NX == 0))
        def _():
            w_down.relay((i - DOWN_AT) // NX)
            w_down.spread((i - DOWN_AT) // NX)

        @pl.when(i < steps - NX)
        def _():
            up_copy(below, below_s, i + NX).start()

        low_copy(above, above_s, i).wait_recv()

        @pl.when((i < steps - NX - half) | ((i >= steps - NX) & (i < steps - half)))
        def _():
            to = jnp.where(i < steps - NX - half, i + NX, i + half)
            low_copy(above, above_s, to).start()

        side_copy(below, below_s, NX + i).start()
        side_copy(above, above_s, NX + steps + i).start()

        @pl.when(i == DOWN_AT)
        def _():
            w_down.begin_across()

        @pl.when((i % 2 == 1) & (i < 2 * mid))
        def _():
            w_out.relay((i + 1) // 2)
            w_out.spread((i + 1) // 2)

        @pl.when((i % 2 == 1) & (i >= OUT_ON))
        def _():
            w_out.onward((i - OUT_ON) // 2)

        @pl.when((i > DOWN_AT) & ((i - DOWN_AT) % NX == 1) & (i >= DOWN_AT + NX))
        def _():
            w_down.onward((i - DOWN_AT) // NX - 1)

        other_b, other_bs = from_below(i - half, 1 - c)
        other_a, other_as = from_above(i - half, 1 - c)
        b_index = jnp.where(i < half, 2 * i, NX + i - half)
        a_index = jnp.where(i < half, 2 * i + 1, NX + steps + i - half)
        side_copy(other_b, other_bs, b_index).wait_recv()
        side_copy(other_a, other_as, a_index).wait_recv()
        attend([(below, below_s), (above, above_s), (other_b, other_bs), (other_a, other_as)])
        return carry

    lax.fori_loop(0, steps, step, 0)
    in_loop = (steps - 1 - DOWN_AT) // NX
    w_out.gather_side(0)
    for k in range((steps - 1 - steps % 2 - OUT_ON) // 2 + 1, mid + 1):
        w_out.onward(k)
    for k in range((steps - 2 - DOWN_AT) // NX, in_loop):
        w_down.onward(k)
    if in_loop < mid - 1:
        w_down.relay(in_loop + 1)
    last = []
    for j in range(steps - half, steps):
        b = from_below(j, 1 - c)
        a = from_above(j, 1 - c)
        side_copy(*b, NX + j).wait_recv()
        side_copy(*a, NX + steps + j).wait_recv()
        last += [b, a]
    for d in order[1:]:
        w_out.gather_side(d)
    attend(last)

    weight = lam_ref[x]
    for j in range(NX):
        a, b = j * tokens, rows + j * tokens
        first = acc[a : a + tokens, :] / jnp.sum(tot[a : a + tokens, :], axis=1, keepdims=True)
        second = acc[b : b + tokens, :] / jnp.sum(tot[b : b + tokens, :], axis=1, keepdims=True)
        diff = first - weight * second
        normal = diff * lax.rsqrt(jnp.mean(diff * diff, axis=1, keepdims=True) + EPS)
        asend[j] = (normal * hgain_ref[...]).astype(BF16)

    my_cols = pl.ds(pl.multiple_of(x * 128, 128), 128)
    a_copies = []
    for d in order[1:]:
        to = (x + d) % NX
        copy = remote(
            asend.at[to],
            arecv.at[:, my_cols],
            as_sem.at[d - 1],
            ar_sem.at[d - 1],
            dev(z, to, c),
        )
        copy.start()
        a_copies.append(copy)
    arecv[:, my_cols] = asend[x]
    if in_loop < mid - 1:
        w_down.spread(in_loop + 1)
    w_out.finish_side()
    for copy in a_copies:
        copy.wait()

    n_rows = res.shape[0]
    width = wo.shape[4]
    hidden_width = wd.shape[4]
    feature_rows = NX * NC * wo.shape[3]

    cols = wo.shape[0] * feature_rows // PARTS
    per_part = nz // PARTS

    def project(rows_ref, weights, k_width, send, recv, s_sem, r_sem):
        copies = []
        for p in range(PARTS):
            at = pl.ds(p * cols, cols)
            w = weights[p * per_part : (p + 1) * per_part].reshape(cols, k_width)
            part = dot_nt(rows_ref[...], w).astype(BF16)
            for t in range(n_tp):
                send[t, :, at] = part[t * n_rows : (t + 1) * n_rows, :]
            for d in range(1, n_tp):
                to = (tp + d) % n_tp
                n = p * (n_tp - 1) + d - 1
                copy = remote(
                    send.at[to, :, at],
                    recv.at[d - 1, :, at],
                    s_sem.at[n],
                    r_sem.at[n],
                    (sp, to),
                )
                copy.start()
                copies.append(copy)
        return copies

    copies = project(arecv, wo, width, psend, precv, ps_sem, pr_sem)
    for k in range(min(in_loop + 2, mid), mid + 1):
        w_down.relay(k)
        w_down.spread(k)
    for k in range(in_loop, mid):
        w_down.onward(k)
    loads[9].wait()
    total = psend[tp].astype(F32)
    for copy in copies:
        copy.wait()
    for d in range(n_tp - 1):
        total = total + precv[d].astype(F32)
    summed = (res[...].astype(F32) + total).astype(BF16)
    after[...] = summed
    stream = summed.astype(F32)
    normal = stream * lax.rsqrt(jnp.mean(stream * stream, axis=1, keepdims=True) + EPS)
    normed = (normal * ngain_ref[...]).astype(BF16)
    nsend[...] = normed
    my_part = pl.ds(pl.multiple_of(tp * n_rows, n_rows), n_rows)
    copies = []
    middle = nsend.shape[1] // 2
    sides = (pl.ds(0, middle), pl.ds(middle, middle))
    for n, side in enumerate(sides):
        for d in range(1, n_tp):
            copy = remote(
                nsend.at[:, side],
                shard.at[my_part, side],
                ns_sem.at[n * (n_tp - 1) + d - 1],
                nr_sem.at[n * (n_tp - 1) + d - 1],
                (sp, (tp + d) % n_tp),
            )
            copy.start()
            copies.append(copy)
    shard[my_part, :] = normed
    w_down.gather_side(0)
    w_down.onward(mid)
    loads[7].wait()
    loads[8].wait()
    tiles = [(lo, min(lo + 256, hidden_width)) for lo in range(0, hidden_width, 256)]
    for copy in copies[: n_tp - 1]:
        copy.wait()
    for lo, hi in tiles:
        left = shard[:, 0:middle]
        gacc[:, lo:hi] = jnp.dot(left, gv[0:middle, lo:hi], preferred_element_type=F32)
        uacc[:, lo:hi] = jnp.dot(left, uv[0:middle, lo:hi], preferred_element_type=F32)
    for copy in copies[n_tp - 1 :]:
        copy.wait()
    w_down.gather_side(1)
    w_down.gather_side(NX - 1)
    for lo, hi in tiles:
        left = shard[:, middle:]
        gate = gacc[:, lo:hi] + jnp.dot(left, gv[middle:, lo:hi], preferred_element_type=F32)
        up = uacc[:, lo:hi] + jnp.dot(left, uv[middle:, lo:hi], preferred_element_type=F32)
        hid[:, lo:hi] = (gate / (1.0 + jnp.exp(-gate)) * up).astype(BF16)
    for d in range(2, NX - 1):
        w_down.gather_side(d)
    w_down.finish_side()

    copies = project(hid, wd, hidden_width, dsend, drecv, fs_sem, fr_sem)

    for d in range(1, NX):
        x_copies[d].wait_send()
    for copy in q_copies:
        copy.wait_send()
    for n in range(steps):
        up_copy(mine, 0, n).wait_send()
        low_copy(mine, 0, n).wait_send()
    for n in range(NX + 2 * steps):
        side_copy(mine, 0, n).wait_send()
    w_out.finish_sends()
    w_down.finish_sends()

    total = dsend[tp].astype(F32)
    for copy in copies:
        copy.wait()
    for d in range(n_tp - 1):
        total = total + drecv[d].astype(F32)
    out_ref[...] = (after[...].astype(F32) + total).astype(BF16)


def local(nz, n_tp, residual, q1, k1, q2, k2, v, lam, head_gain, out_w, norm_gain, gate, up, down):
    tokens = q1.shape[0]
    rows = NX * tokens
    n_rows, features = residual.shape
    hidden = gate.shape[1]
    steps = NX * (nz - 1) // 2
    mid = nz // 2
    vmem = pl.BlockSpec(memory_space=pltpu.VMEM)
    smem = pl.BlockSpec(memory_space=pltpu.SMEM)
    hbm = pl.BlockSpec(memory_space=pl.ANY)
    dma = pltpu.SemaphoreType.DMA

    def like(a):
        return pltpu.VMEM(a.shape, a.dtype)

    return pl.pallas_call(
        functools.partial(kernel, nz, n_tp),
        out_shape=jax.ShapeDtypeStruct((n_rows, features), BF16),
        in_specs=[hbm] * 6 + [smem, vmem, hbm, vmem, hbm, hbm, hbm],
        out_specs=vmem,
        scratch_shapes=[
            like(residual),
            like(q1),
            like(k1),
            like(q2),
            like(k2),
            like(v),
            like(gate),
            like(up),
            pltpu.VMEM((nz, NX, NC, *out_w.shape), BF16),
            pltpu.VMEM((nz, NX, NC, *down.shape), BF16),
            pltpu.VMEM((NX, tokens, 128), BF16),
            pltpu.VMEM((NX, 2, tokens, 128), BF16),
            pltpu.VMEM((rows, 128), BF16),
            pltpu.VMEM((2 * rows, 128), BF16),
            pltpu.VMEM((nz * NC, 2, rows, 128), BF16),
            pltpu.VMEM((2 * rows, 128), F32),
            pltpu.VMEM((2 * rows, 128), F32),
            pltpu.VMEM((2 * rows, 128), F32),
            pltpu.VMEM((NX, tokens, 128), BF16),
            pltpu.VMEM((tokens, NX * 128), BF16),
            pltpu.VMEM((n_tp, n_rows, features), BF16),
            pltpu.VMEM((n_tp - 1, n_rows, features), BF16),
            pltpu.VMEM((n_rows, features), BF16),
            pltpu.VMEM((n_rows, features), BF16),
            pltpu.VMEM((tokens, features), BF16),
            pltpu.VMEM((tokens, hidden), F32),
            pltpu.VMEM((tokens, hidden), F32),
            pltpu.VMEM((tokens, hidden), BF16),
            pltpu.VMEM((n_tp, n_rows, features), BF16),
            pltpu.VMEM((n_tp - 1, n_rows, features), BF16),
            dma((10,)),
            dma((2 * (NX - 1),)),
            dma((2 * (NX - 1),)),
            dma((steps,)),
            dma((steps,)),
            dma((steps,)),
            dma((steps,)),
            dma((NX + 2 * steps,)),
            dma((NX + 2 * steps,)),
            dma((NX - 1,)),
            dma((NX - 1,)),
            dma((2 * mid,)),
            dma((2 * mid,)),
            dma((2 * mid,)),
            dma((2 * mid,)),
            dma((2 * (NX - 1) * nz,)),
            dma((2 * (NX - 1) * nz,)),
            dma((2 * NX,)),
            dma((2 * NX,)),
            dma((PARTS * (n_tp - 1),)),
            dma((PARTS * (n_tp - 1),)),
            dma((2 * (n_tp - 1),)),
            dma((2 * (n_tp - 1),)),
            dma((PARTS * (n_tp - 1),)),
            dma((PARTS * (n_tp - 1),)),
        ],
        compiler_params=pltpu.CompilerParams(
            collective_id=0, has_side_effects=True, vmem_limit_bytes=62 * 2**20
        ),
        name="layer",
    )(
        residual,
        q1,
        k1,
        q2,
        k2,
        v,
        lam,
        head_gain.reshape(1, 128),
        out_w,
        norm_gain.reshape(1, features),
        gate,
        up,
        down,
    )


def solution(mesh):
    nz = mesh.shape["sp"] // (NX * NC)
    n_tp = mesh.shape["tp"]
    return jax.shard_map(
        functools.partial(local, nz, n_tp),
        mesh=mesh,
        in_specs=(
            P(("sp", "tp"), None),
            P("sp", "tp"),
            P("sp", "tp"),
            P("sp", "tp"),
            P("sp", "tp"),
            P("sp", "tp"),
            P("tp"),
            P(),
            P("sp", "tp"),
            P(),
            P(None, "tp"),
            P(None, "tp"),
            P("sp", "tp"),
        ),
        out_specs=P(("sp", "tp"), None),
        check_vma=False,
    )
```

```python
import functools
import math

import jax
import jax.numpy as jnp
from jax import lax
from jax.experimental import pallas as pl
from jax.experimental.pallas import tpu as pltpu
from jax.sharding import PartitionSpec as P

EPS = 1e-06
MESH = pl.DeviceIdType.MESH
NX = 4
NC = 2
DOWN_AT = 6
OUT_ON = 5
PARTS = 2
F32 = jnp.float32
BF16 = jnp.bfloat16


def dot_nt(a, b):
    return lax.dot_general(a, b, (((1,), (1,)), ((), ())), preferred_element_type=F32)


def remote(src, dst, send, recv, device):
    return pltpu.make_async_remote_copy(
        src_ref=src,
        dst_ref=dst,
        send_sem=send,
        recv_sem=recv,
        device_id=device,
        device_id_type=MESH,
    )


def kernel(
    nz,
    n_tp,
    res_hbm,
    q1_hbm,
    k1_hbm,
    q2_hbm,
    k2_hbm,
    v_hbm,
    lam_ref,
    hgain_ref,
    outw_hbm,
    ngain_ref,
    gate_hbm,
    up_hbm,
    downw_hbm,
    out_ref,
    res,
    q1,
    k1,
    q2,
    k2,
    v,
    gv,
    uv,
    wo,
    wd,
    packq,
    packkv,
    qrecv,
    qs,
    kv,
    acc,
    mx,
    tot,
    asend,
    arecv,
    psend,
    precv,
    after,
    nsend,
    shard,
    gacc,
    uacc,
    hid,
    dsend,
    drecv,
    load_sem,
    xs_sem,
    xr_sem,
    us_sem,
    ur_sem,
    ls_sem,
    lr_sem,
    ds_sem,
    dr_sem,
    as_sem,
    ar_sem,
    wus_sem,
    wur_sem,
    wls_sem,
    wlr_sem,
    wxs_sem,
    wxr_sem,
    wds_sem,
    wdr_sem,
    ps_sem,
    pr_sem,
    ns_sem,
    nr_sem,
    fs_sem,
    fr_sem,
):
    sp = lax.axis_index("sp")
    tp = lax.axis_index("tp")
    z = sp // (NX * NC)
    x = (sp // NC) % NX
    c = sp % NC
    tokens = q1.shape[0]
    rows = NX * tokens
    steps = NX * (nz - 1) // 2
    mid = nz // 2
    half = NX // 2

    def dev(zz, xx, cc):
        return ((zz * NX + xx) * NC + cc, tp)

    z_up = (z + 1) % nz
    z_dn = (z + nz - 1) % nz
    other = dev(z, x, 1 - c)

    loads = []
    for n, (src, dst) in enumerate(
        (
            (k1_hbm, k1),
            (k2_hbm, k2),
            (v_hbm, v),
            (q1_hbm, q1),
            (q2_hbm, q2),
            (outw_hbm, wo.at[z, x, c]),
            (downw_hbm, wd.at[z, x, c]),
            (gate_hbm, gv),
            (up_hbm, uv),
            (res_hbm, res),
        )
    ):
        load = pltpu.make_async_copy(src, dst, load_sem.at[n])
        load.start()
        loads.append(load)

    peers = [dev(z, (x + d) % NX, c) for d in range(1, NX)]
    peers += [dev(z_up, x, c), dev(z_dn, x, c), other]
    peers += [(sp, (tp + d) % n_tp) for d in range(1, n_tp)]
    barrier = pltpu.get_barrier_semaphore()
    for p in peers:
        pl.semaphore_signal(barrier, inc=1, device_id=p, device_id_type=MESH)

    low = lax.broadcasted_iota(jnp.int32, (tokens, 128), 1) < 64

    def joined(first, second, j):
        a = first[:, 128 * (j // 2) : 128 * (j // 2) + 128].astype(F32)
        b = second[:, 128 * (j // 2) : 128 * (j // 2) + 128].astype(F32)
        if j % 2 == 0:
            b = pltpu.roll(b, 64, 1)
        else:
            a = pltpu.roll(a, 64, 1)
        return jnp.where(low, a, b).astype(BF16)

    mine = z * NC + c
    my_rows = pl.ds(pl.multiple_of(x * tokens, tokens), tokens)
    for load in loads[:3]:
        load.wait()
    for j in range(NX):
        packkv[j, 0] = joined(k1, k2, j)
        packkv[j, 1] = v[:, 128 * j : 128 * j + 128]
    kv[mine, :, my_rows, :] = packkv[x]
    for load in loads[3:5]:
        load.wait()
    for j in range(NX):
        packq[j] = joined(q1, q2, j)
    qrecv[my_rows, :] = packq[x]
    pl.semaphore_wait(barrier, len(peers))

    order = [0, 1, NX - 1] + list(range(2, NX - 1))

    def source(s):
        back = s
        for n, d in enumerate(order):
            back = jnp.where(s == n, d, back)
        return (x + NX - back) % NX

    def piece(slot, s):
        at = pl.multiple_of(source(s) * tokens, tokens)
        return kv.at[slot, :, pl.ds(at, tokens), :]

    def up_copy(slot, s, index):
        part = piece(slot, s)
        return remote(part, part, us_sem.at[index], ur_sem.at[index], dev(z_up, x, c))

    def low_copy(slot, s, index):
        part = piece(slot, s)
        return remote(part, part, ls_sem.at[index], lr_sem.at[index], dev(z_dn, x, c))

    def side_copy(slot, s, index):
        part = piece(slot, s)
        return remote(part, part, ds_sem.at[index], dr_sem.at[index], other)

    def from_below(j, core):
        d = (j + NX) // NX
        s = jnp.where(j < 0, 2 * (j + half), (j + NX) % NX)
        return ((z + nz - d) % nz) * NC + core, s

    def from_above(j, core):
        d = (j + NX) // NX
        s = (j + NX) % NX
        s = jnp.where(j < 0, 2 * (j + half) + 1, jnp.where(j >= steps - half, s + half, s))
        return ((z + d) % nz) * NC + core, s

    class Weight:
        def __init__(self, ref, n):
            self.ref = ref
            self.n = n

        def up(self, zz, k):
            block = self.ref.at[zz, x, c]
            at = self.n * mid + k - 1
            return remote(block, block, wus_sem.at[at], wur_sem.at[at], dev(z_up, x, c))

        def low(self, zz, k):
            block = self.ref.at[zz, x, c]
            at = self.n * mid + k - 1
            return remote(block, block, wls_sem.at[at], wlr_sem.at[at], dev(z_dn, x, c))

        def across(self, zz, d):
            block = self.ref.at[zz, x, c]
            at = (self.n * (NX - 1) + d - 1) * nz + zz
            return remote(block, block, wxs_sem.at[at], wxr_sem.at[at], dev(z, (x + d) % NX, c))

        def side(self, d):
            block = self.ref.at[:, (x + NX - d) % NX, c]
            at = self.n * NX + d
            return remote(block, block, wds_sem.at[at], wdr_sem.at[at], other)

        def begin(self):
            self.up(z, 1).start()
            self.low(z, 1).start()

        def begin_across(self):
            self.across(z, 1).start()
            self.across(z, NX - 1).start()

        def relay(self, k):
            below = (z + nz - k) % nz
            above = (z + k) % nz

            @pl.when((k < mid) | (c == 0))
            def _():
                self.up(below, k).wait_recv()

            @pl.when((k < mid) | (c == 1))
            def _():
                self.low(above, k).wait_recv()

            @pl.when((k < mid - 1) | ((k == mid - 1) & (c == 0)))
            def _():
                self.up(below, k + 1).start()

            @pl.when((k < mid - 1) | ((k == mid - 1) & (c == 1)))
            def _():
                self.low(above, k + 1).start()

        def spread(self, k):
            below = (z + nz - k) % nz
            above = (z + k) % nz
            for d in (1, NX - 1):
                self.across(below, d).start()

            @pl.when(k < mid)
            def _():
                for d in (1, NX - 1):
                    self.across(above, d).start()

        def second(self, zz, d):
            block = self.ref.at[zz, (x + NX - d) % NX, c]
            at = (self.n * (NX - 1) + 1) * nz + zz
            return remote(block, block, wxs_sem.at[at], wxr_sem.at[at], dev(z, (x + d) % NX, c))

        def onward(self, k):
            below = (z + nz - k) % nz
            above = (z + k) % nz
            both = (k > 0) & (k < mid)

            @pl.when(both | (c == 0))
            def _():
                self.across(below, 1).wait_recv()
                self.second(below, 1).start()

            @pl.when(both | (c == 1))
            def _():
                self.across(above, NX - 1).wait_recv()
                self.second(above, NX - 1).start()

        def gather_side(self, d):
            if d == 1 or d == NX - 1:
                for k in range(1, mid):
                    zz = (z + k) % nz if d == 1 else (z + nz - k) % nz
                    self.across(zz, d).wait_recv()

                @pl.when(c == (1 if d == 1 else 0))
                def _():
                    self.across(z, d).wait_recv()
                    self.across((z + mid) % nz, d).wait_recv()

            elif d:
                for zz in range(nz):
                    self.across(zz, d).wait_recv()
            self.side(d).start()

        def finish_side(self):
            for d in range(NX):
                self.side(d).wait_recv()

        def finish_sends(self):
            for k in range(1, mid):
                self.up(z, k).wait_send()
                self.low(z, k).wait_send()

            @pl.when(c == 0)
            def _():
                self.up(z, mid).wait_send()

            @pl.when(c == 1)
            def _():
                self.low(z, mid).wait_send()

            for d in range(1, NX):
                for zz in range(nz):
                    self.across(zz, d).wait_send()
            for d in range(NX):
                self.side(d).wait_send()

    w_out = Weight(wo, 0)
    w_down = Weight(wd, 1)
    up_copy(mine, 0, 0).start()
    low_copy(mine, 0, 0).start()
    side_copy(mine, 0, 0).start()
    x_copies = {}
    for d in order[1:]:
        to = (x + d) % NX
        x_copies[d] = remote(
            packkv.at[to],
            kv.at[mine, :, my_rows, :],
            xs_sem.at[d - 1],
            xr_sem.at[d - 1],
            dev(z, to, c),
        )
        x_copies[d].start()
    q_copies = []
    for d in order[1:]:
        to = (x + d) % NX
        copy = remote(
            packq.at[to],
            qrecv.at[my_rows, :],
            xs_sem.at[NX + d - 2],
            xr_sem.at[NX + d - 2],
            dev(z, to, c),
        )
        copy.start()
        q_copies.append(copy)
    for s, d in enumerate(order[1:], 1):
        x_copies[d].wait_recv()
        up_copy(mine, s, s).start()
        low_copy(mine, s, s).start()
        side_copy(mine, s, s).start()

    loads[5].wait()
    w_out.begin()
    w_out.begin_across()
    acc[...] = jnp.zeros_like(acc)
    tot[...] = jnp.zeros_like(tot)
    mx[...] = jnp.full(mx.shape, -3e38, F32)
    for copy in q_copies:
        copy.wait_recv()
    lane = lax.broadcasted_iota(jnp.int32, (rows, 128), 1) < 64
    queries = qrecv[...].astype(F32)
    qs[0:rows, :] = jnp.where(lane, queries, 0.0).astype(BF16)
    qs[rows : 2 * rows, :] = jnp.where(lane, 0.0, queries).astype(BF16)
    loads[6].wait()

    scale = 64 ** (-0.5) * math.log2(math.e)
    tile = rows

    def attend(blocks):
        width = len(blocks) * tokens
        keys = jnp.concatenate([piece(slot, s)[0] for slot, s in blocks], axis=0)
        vals = jnp.concatenate([piece(slot, s)[1] for slot, s in blocks], axis=0)
        halves = [pl.ds(n * tile, tile) for n in range(2)]
        for at, scores in [(at, dot_nt(qs[at, :], keys)) for at in halves]:
            old = mx[at, :]
            top = scores[:, 0:128]
            for lo in range(128, width, 128):
                top = jnp.maximum(top, scores[:, lo : lo + 128])
            new = jnp.maximum(old, jnp.max(top, axis=1, keepdims=True))
            factor = jnp.exp2((old - new) * scale)
            total = tot[at, :] * factor
            parts = []
            for lo in range(0, width, 128):
                part = jnp.exp2((scores[:, lo : lo + 128] - new) * scale)
                total = total + part
                parts.append(part.astype(BF16))
            mx[at, :] = new
            tot[at, :] = total
            acc[at, :] = acc[at, :] * factor + jnp.dot(
                jnp.concatenate(parts, axis=1), vals, preferred_element_type=F32
            )

    attend([(mine, s) for s in range(NX)])

    def step(i, carry):
        below, below_s = from_below(i, c)
        above, above_s = from_above(i, c)
        up_copy(below, below_s, i).wait_recv()

        @pl.when(i == DOWN_AT)
        def _():
            w_down.begin()

        @pl.when((i > DOWN_AT) & ((i - DOWN_AT) % NX == 0))
        def _():
            w_down.relay((i - DOWN_AT) // NX)
            w_down.spread((i - DOWN_AT) // NX)

        @pl.when(i < steps - NX)
        def _():
            up_copy(below, below_s, i + NX).start()

        low_copy(above, above_s, i).wait_recv()

        @pl.when((i < steps - NX - half) | ((i >= steps - NX) & (i < steps - half)))
        def _():
            to = jnp.where(i < steps - NX - half, i + NX, i + half)
            low_copy(above, above_s, to).start()

        side_copy(below, below_s, NX + i).start()
        side_copy(above, above_s, NX + steps + i).start()

        @pl.when(i == 3)
        def _():
            w_down.begin_across()

        @pl.when((i % 2 == 1) & (i < 2 * mid))
        def _():
            w_out.relay((i + 1) // 2)
            w_out.spread((i + 1) // 2)

        @pl.when((i % 2 == 1) & (i >= OUT_ON))
        def _():
            w_out.onward((i - OUT_ON) // 2)

        @pl.when((i > DOWN_AT) & ((i - DOWN_AT) % NX == 1) & (i >= DOWN_AT + NX))
        def _():
            w_down.onward((i - DOWN_AT) // NX - 1)

        other_b, other_bs = from_below(i - half, 1 - c)
        other_a, other_as = from_above(i - half, 1 - c)
        b_index = jnp.where(i < half, 2 * i, NX + i - half)
        a_index = jnp.where(i < half, 2 * i + 1, NX + steps + i - half)
        side_copy(other_b, other_bs, b_index).wait_recv()
        side_copy(other_a, other_as, a_index).wait_recv()
        attend([(below, below_s), (above, above_s), (other_b, other_bs), (other_a, other_as)])
        return carry

    lax.fori_loop(0, steps, step, 0)
    in_loop = (steps - 1 - DOWN_AT) // NX
    w_out.gather_side(0)
    for k in range((steps - 1 - steps % 2 - OUT_ON) // 2 + 1, mid + 1):
        w_out.onward(k)
    for k in range((steps - 2 - DOWN_AT) // NX, in_loop):
        w_down.onward(k)
    if in_loop < mid - 1:
        w_down.relay(in_loop + 1)
    last = []
    for j in range(steps - half, steps):
        b = from_below(j, 1 - c)
        a = from_above(j, 1 - c)
        side_copy(*b, NX + j).wait_recv()
        side_copy(*a, NX + steps + j).wait_recv()
        last += [b, a]
    for d in order[1:]:
        w_out.gather_side(d)
    attend(last)

    weight = lam_ref[x]
    for j in range(NX):
        a, b = j * tokens, rows + j * tokens
        first = acc[a : a + tokens, :] / jnp.sum(tot[a : a + tokens, :], axis=1, keepdims=True)
        second = acc[b : b + tokens, :] / jnp.sum(tot[b : b + tokens, :], axis=1, keepdims=True)
        diff = first - weight * second
        normal = diff * lax.rsqrt(jnp.mean(diff * diff, axis=1, keepdims=True) + EPS)
        asend[j] = (normal * hgain_ref[...]).astype(BF16)

    my_cols = pl.ds(pl.multiple_of(x * 128, 128), 128)
    a_copies = []
    for d in order[1:]:
        to = (x + d) % NX
        copy = remote(
            asend.at[to],
            arecv.at[:, my_cols],
            as_sem.at[d - 1],
            ar_sem.at[d - 1],
            dev(z, to, c),
        )
        copy.start()
        a_copies.append(copy)
    arecv[:, my_cols] = asend[x]
    if in_loop < mid - 1:
        w_down.spread(in_loop + 1)
    w_out.finish_side()
    for copy in a_copies:
        copy.wait()

    n_rows = res.shape[0]
    width = wo.shape[4]
    hidden_width = wd.shape[4]
    feature_rows = NX * NC * wo.shape[3]

    cols = wo.shape[0] * feature_rows // PARTS
    per_part = nz // PARTS

    def project(rows_ref, weights, k_width, send, recv, s_sem, r_sem):
        copies = []
        for p in range(PARTS):
            at = pl.ds(p * cols, cols)
            w = weights[p * per_part : (p + 1) * per_part].reshape(cols, k_width)
            part = dot_nt(rows_ref[...], w).astype(BF16)
            for t in range(n_tp):
                send[t, :, at] = part[t * n_rows : (t + 1) * n_rows, :]
            for d in range(1, n_tp):
                to = (tp + d) % n_tp
                n = p * (n_tp - 1) + d - 1
                copy = remote(
                    send.at[to, :, at],
                    recv.at[d - 1, :, at],
                    s_sem.at[n],
                    r_sem.at[n],
                    (sp, to),
                )
                copy.start()
                copies.append(copy)
        return copies

    copies = project(arecv, wo, width, psend, precv, ps_sem, pr_sem)
    for k in range(min(in_loop + 2, mid), mid + 1):
        w_down.relay(k)
        w_down.spread(k)
    for k in range(in_loop, mid):
        w_down.onward(k)
    loads[9].wait()
    total = psend[tp].astype(F32)
    for copy in copies:
        copy.wait()
    for d in range(n_tp - 1):
        total = total + precv[d].astype(F32)
    summed = (res[...].astype(F32) + total).astype(BF16)
    after[...] = summed
    stream = summed.astype(F32)
    normal = stream * lax.rsqrt(jnp.mean(stream * stream, axis=1, keepdims=True) + EPS)
    normed = (normal * ngain_ref[...]).astype(BF16)
    nsend[...] = normed
    my_part = pl.ds(pl.multiple_of(tp * n_rows, n_rows), n_rows)
    copies = []
    middle = nsend.shape[1] // 2
    sides = (pl.ds(0, middle), pl.ds(middle, middle))
    for n, side in enumerate(sides):
        for d in range(1, n_tp):
            copy = remote(
                nsend.at[:, side],
                shard.at[my_part, side],
                ns_sem.at[n * (n_tp - 1) + d - 1],
                nr_sem.at[n * (n_tp - 1) + d - 1],
                (sp, (tp + d) % n_tp),
            )
            copy.start()
            copies.append(copy)
    shard[my_part, :] = normed
    w_down.gather_side(0)
    w_down.onward(mid)
    loads[7].wait()
    loads[8].wait()
    tiles = [(lo, min(lo + 256, hidden_width)) for lo in range(0, hidden_width, 256)]
    for copy in copies[: n_tp - 1]:
        copy.wait()
    w_down.gather_side(1)
    w_down.gather_side(NX - 1)
    for lo, hi in tiles:
        left = shard[:, 0:middle]
        gacc[:, lo:hi] = jnp.dot(left, gv[0:middle, lo:hi], preferred_element_type=F32)
        uacc[:, lo:hi] = jnp.dot(left, uv[0:middle, lo:hi], preferred_element_type=F32)
    for copy in copies[n_tp - 1 :]:
        copy.wait()
    for lo, hi in tiles:
        left = shard[:, middle:]
        gate = gacc[:, lo:hi] + jnp.dot(left, gv[middle:, lo:hi], preferred_element_type=F32)
        up = uacc[:, lo:hi] + jnp.dot(left, uv[middle:, lo:hi], preferred_element_type=F32)
        hid[:, lo:hi] = (gate / (1.0 + jnp.exp(-gate)) * up).astype(BF16)
    for d in range(2, NX - 1):
        w_down.gather_side(d)
    w_down.finish_side()

    copies = project(hid, wd, hidden_width, dsend, drecv, fs_sem, fr_sem)

    for d in range(1, NX):
        x_copies[d].wait_send()
    for copy in q_copies:
        copy.wait_send()
    for n in range(steps):
        up_copy(mine, 0, n).wait_send()
        low_copy(mine, 0, n).wait_send()
    for n in range(NX + 2 * steps):
        side_copy(mine, 0, n).wait_send()
    w_out.finish_sends()
    w_down.finish_sends()

    total = dsend[tp].astype(F32)
    for copy in copies:
        copy.wait()
    for d in range(n_tp - 1):
        total = total + drecv[d].astype(F32)
    out_ref[...] = (after[...].astype(F32) + total).astype(BF16)


def local(nz, n_tp, residual, q1, k1, q2, k2, v, lam, head_gain, out_w, norm_gain, gate, up, down):
    tokens = q1.shape[0]
    rows = NX * tokens
    n_rows, features = residual.shape
    hidden = gate.shape[1]
    steps = NX * (nz - 1) // 2
    mid = nz // 2
    vmem = pl.BlockSpec(memory_space=pltpu.VMEM)
    smem = pl.BlockSpec(memory_space=pltpu.SMEM)
    hbm = pl.BlockSpec(memory_space=pl.ANY)
    dma = pltpu.SemaphoreType.DMA

    def like(a):
        return pltpu.VMEM(a.shape, a.dtype)

    return pl.pallas_call(
        functools.partial(kernel, nz, n_tp),
        out_shape=jax.ShapeDtypeStruct((n_rows, features), BF16),
        in_specs=[hbm] * 6 + [smem, vmem, hbm, vmem, hbm, hbm, hbm],
        out_specs=vmem,
        scratch_shapes=[
            like(residual),
            like(q1),
            like(k1),
            like(q2),
            like(k2),
            like(v),
            like(gate),
            like(up),
            pltpu.VMEM((nz, NX, NC, *out_w.shape), BF16),
            pltpu.VMEM((nz, NX, NC, *down.shape), BF16),
            pltpu.VMEM((NX, tokens, 128), BF16),
            pltpu.VMEM((NX, 2, tokens, 128), BF16),
            pltpu.VMEM((rows, 128), BF16),
            pltpu.VMEM((2 * rows, 128), BF16),
            pltpu.VMEM((nz * NC, 2, rows, 128), BF16),
            pltpu.VMEM((2 * rows, 128), F32),
            pltpu.VMEM((2 * rows, 128), F32),
            pltpu.VMEM((2 * rows, 128), F32),
            pltpu.VMEM((NX, tokens, 128), BF16),
            pltpu.VMEM((tokens, NX * 128), BF16),
            pltpu.VMEM((n_tp, n_rows, features), BF16),
            pltpu.VMEM((n_tp - 1, n_rows, features), BF16),
            pltpu.VMEM((n_rows, features), BF16),
            pltpu.VMEM((n_rows, features), BF16),
            pltpu.VMEM((tokens, features), BF16),
            pltpu.VMEM((tokens, hidden), F32),
            pltpu.VMEM((tokens, hidden), F32),
            pltpu.VMEM((tokens, hidden), BF16),
            pltpu.VMEM((n_tp, n_rows, features), BF16),
            pltpu.VMEM((n_tp - 1, n_rows, features), BF16),
            dma((10,)),
            dma((2 * (NX - 1),)),
            dma((2 * (NX - 1),)),
            dma((steps,)),
            dma((steps,)),
            dma((steps,)),
            dma((steps,)),
            dma((NX + 2 * steps,)),
            dma((NX + 2 * steps,)),
            dma((NX - 1,)),
            dma((NX - 1,)),
            dma((2 * mid,)),
            dma((2 * mid,)),
            dma((2 * mid,)),
            dma((2 * mid,)),
            dma((2 * (NX - 1) * nz,)),
            dma((2 * (NX - 1) * nz,)),
            dma((2 * NX,)),
            dma((2 * NX,)),
            dma((PARTS * (n_tp - 1),)),
            dma((PARTS * (n_tp - 1),)),
            dma((2 * (n_tp - 1),)),
            dma((2 * (n_tp - 1),)),
            dma((PARTS * (n_tp - 1),)),
            dma((PARTS * (n_tp - 1),)),
        ],
        compiler_params=pltpu.CompilerParams(
            collective_id=0, has_side_effects=True, vmem_limit_bytes=62 * 2**20
        ),
        name="layer",
    )(
        residual,
        q1,
        k1,
        q2,
        k2,
        v,
        lam,
        head_gain.reshape(1, 128),
        out_w,
        norm_gain.reshape(1, features),
        gate,
        up,
        down,
    )


def solution(mesh):
    nz = mesh.shape["sp"] // (NX * NC)
    n_tp = mesh.shape["tp"]
    return jax.shard_map(
        functools.partial(local, nz, n_tp),
        mesh=mesh,
        in_specs=(
            P(("sp", "tp"), None),
            P("sp", "tp"),
            P("sp", "tp"),
            P("sp", "tp"),
            P("sp", "tp"),
            P("sp", "tp"),
            P("tp"),
            P(),
            P("sp", "tp"),
            P(),
            P(None, "tp"),
            P(None, "tp"),
            P("sp", "tp"),
        ),
        out_specs=P(("sp", "tp"), None),
        check_vma=False,
    )
```

```python
import functools
import math

import jax
import jax.numpy as jnp
from jax import lax
from jax.experimental import pallas as pl
from jax.experimental.pallas import tpu as pltpu
from jax.sharding import PartitionSpec as P

EPS = 1e-06
MESH = pl.DeviceIdType.MESH
NX = 4
NC = 2
DOWN_AT = 6
OUT_ON = 5
PARTS = 4
F32 = jnp.float32
BF16 = jnp.bfloat16


def dot_nt(a, b):
    return lax.dot_general(a, b, (((1,), (1,)), ((), ())), preferred_element_type=F32)


def remote(src, dst, send, recv, device):
    return pltpu.make_async_remote_copy(
        src_ref=src,
        dst_ref=dst,
        send_sem=send,
        recv_sem=recv,
        device_id=device,
        device_id_type=MESH,
    )


def kernel(
    nz,
    n_tp,
    res_hbm,
    q1_hbm,
    k1_hbm,
    q2_hbm,
    k2_hbm,
    v_hbm,
    lam_ref,
    hgain_ref,
    outw_hbm,
    ngain_ref,
    gate_hbm,
    up_hbm,
    downw_hbm,
    out_ref,
    res,
    q1,
    k1,
    q2,
    k2,
    v,
    gv,
    uv,
    wo,
    wd,
    packq,
    packkv,
    qrecv,
    qs,
    kv,
    acc,
    mx,
    tot,
    asend,
    arecv,
    psend,
    precv,
    after,
    nsend,
    shard,
    gacc,
    uacc,
    hid,
    dsend,
    drecv,
    load_sem,
    xs_sem,
    xr_sem,
    us_sem,
    ur_sem,
    ls_sem,
    lr_sem,
    ds_sem,
    dr_sem,
    as_sem,
    ar_sem,
    wus_sem,
    wur_sem,
    wls_sem,
    wlr_sem,
    wxs_sem,
    wxr_sem,
    wds_sem,
    wdr_sem,
    ps_sem,
    pr_sem,
    ns_sem,
    nr_sem,
    fs_sem,
    fr_sem,
):
    sp = lax.axis_index("sp")
    tp = lax.axis_index("tp")
    z = sp // (NX * NC)
    x = (sp // NC) % NX
    c = sp % NC
    tokens = q1.shape[0]
    rows = NX * tokens
    steps = NX * (nz - 1) // 2
    mid = nz // 2
    half = NX // 2

    def dev(zz, xx, cc):
        return ((zz * NX + xx) * NC + cc, tp)

    z_up = (z + 1) % nz
    z_dn = (z + nz - 1) % nz
    other = dev(z, x, 1 - c)

    loads = []
    for n, (src, dst) in enumerate(
        (
            (k1_hbm, k1),
            (k2_hbm, k2),
            (v_hbm, v),
            (q1_hbm, q1),
            (q2_hbm, q2),
            (outw_hbm, wo.at[z, x, c]),
            (downw_hbm, wd.at[z, x, c]),
            (gate_hbm, gv),
            (up_hbm, uv),
            (res_hbm, res),
        )
    ):
        load = pltpu.make_async_copy(src, dst, load_sem.at[n])
        load.start()
        loads.append(load)

    peers = [dev(z, (x + d) % NX, c) for d in range(1, NX)]
    peers += [dev(z_up, x, c), dev(z_dn, x, c), other]
    peers += [(sp, (tp + d) % n_tp) for d in range(1, n_tp)]
    barrier = pltpu.get_barrier_semaphore()
    for p in peers:
        pl.semaphore_signal(barrier, inc=1, device_id=p, device_id_type=MESH)

    low = lax.broadcasted_iota(jnp.int32, (tokens, 128), 1) < 64

    def joined(first, second, j):
        a = first[:, 128 * (j // 2) : 128 * (j // 2) + 128].astype(F32)
        b = second[:, 128 * (j // 2) : 128 * (j // 2) + 128].astype(F32)
        if j % 2 == 0:
            b = pltpu.roll(b, 64, 1)
        else:
            a = pltpu.roll(a, 64, 1)
        return jnp.where(low, a, b).astype(BF16)

    mine = z * NC + c
    my_rows = pl.ds(pl.multiple_of(x * tokens, tokens), tokens)
    for load in loads[:3]:
        load.wait()
    for j in range(NX):
        packkv[j, 0] = joined(k1, k2, j)
        packkv[j, 1] = v[:, 128 * j : 128 * j + 128]
    kv[mine, :, my_rows, :] = packkv[x]
    for load in loads[3:5]:
        load.wait()
    for j in range(NX):
        packq[j] = joined(q1, q2, j)
    qrecv[my_rows, :] = packq[x]
    pl.semaphore_wait(barrier, len(peers))

    order = [0, 1, NX - 1] + list(range(2, NX - 1))

    def source(s):
        back = s
        for n, d in enumerate(order):
            back = jnp.where(s == n, d, back)
        return (x + NX - back) % NX

    def piece(slot, s):
        at = pl.multiple_of(source(s) * tokens, tokens)
        return kv.at[slot, :, pl.ds(at, tokens), :]

    def up_copy(slot, s, index):
        part = piece(slot, s)
        return remote(part, part, us_sem.at[index], ur_sem.at[index], dev(z_up, x, c))

    def low_copy(slot, s, index):
        part = piece(slot, s)
        return remote(part, part, ls_sem.at[index], lr_sem.at[index], dev(z_dn, x, c))

    def side_copy(slot, s, index):
        part = piece(slot, s)
        return remote(part, part, ds_sem.at[index], dr_sem.at[index], other)

    def from_below(j, core):
        d = (j + NX) // NX
        s = jnp.where(j < 0, 2 * (j + half), (j + NX) % NX)
        return ((z + nz - d) % nz) * NC + core, s

    def from_above(j, core):
        d = (j + NX) // NX
        s = (j + NX) % NX
        s = jnp.where(j < 0, 2 * (j + half) + 1, jnp.where(j >= steps - half, s + half, s))
        return ((z + d) % nz) * NC + core, s

    class Weight:
        def __init__(self, ref, n):
            self.ref = ref
            self.n = n

        def up(self, zz, k):
            block = self.ref.at[zz, x, c]
            at = self.n * mid + k - 1
            return remote(block, block, wus_sem.at[at], wur_sem.at[at], dev(z_up, x, c))

        def low(self, zz, k):
            block = self.ref.at[zz, x, c]
            at = self.n * mid + k - 1
            return remote(block, block, wls_sem.at[at], wlr_sem.at[at], dev(z_dn, x, c))

        def across(self, zz, d):
            block = self.ref.at[zz, x, c]
            at = (self.n * (NX - 1) + d - 1) * nz + zz
            return remote(block, block, wxs_sem.at[at], wxr_sem.at[at], dev(z, (x + d) % NX, c))

        def side(self, d):
            block = self.ref.at[:, (x + NX - d) % NX, c]
            at = self.n * NX + d
            return remote(block, block, wds_sem.at[at], wdr_sem.at[at], other)

        def begin(self):
            self.up(z, 1).start()
            self.low(z, 1).start()

        def begin_across(self):
            self.across(z, 1).start()
            self.across(z, NX - 1).start()

        def relay(self, k):
            below = (z + nz - k) % nz
            above = (z + k) % nz
            after_k = jnp.minimum(k + 1, mid)

            @pl.when((k < mid) | (c == 0))
            def _():
                self.up(below, k).wait_recv()

            @pl.when((k < mid) | (c == 1))
            def _():
                self.low(above, k).wait_recv()

            @pl.when((k < mid - 1) | ((k == mid - 1) & (c == 0)))
            def _():
                self.up(below, after_k).start()

            @pl.when((k < mid - 1) | ((k == mid - 1) & (c == 1)))
            def _():
                self.low(above, after_k).start()

        def spread(self, k):
            below = (z + nz - k) % nz
            above = (z + k) % nz
            for d in (1, NX - 1):
                self.across(below, d).start()

            @pl.when(k < mid)
            def _():
                for d in (1, NX - 1):
                    self.across(above, d).start()

        def second(self, zz, d):
            block = self.ref.at[zz, (x + NX - d) % NX, c]
            at = (self.n * (NX - 1) + 1) * nz + zz
            return remote(block, block, wxs_sem.at[at], wxr_sem.at[at], dev(z, (x + d) % NX, c))

        def onward(self, k):
            below = (z + nz - k) % nz
            above = (z + k) % nz
            both = (k > 0) & (k < mid)

            @pl.when(both | (c == 0))
            def _():
                self.across(below, 1).wait_recv()
                self.second(below, 1).start()

            @pl.when(both | (c == 1))
            def _():
                self.across(above, NX - 1).wait_recv()
                self.second(above, NX - 1).start()

        def gather_side(self, d):
            if d == 1 or d == NX - 1:
                for k in range(1, mid):
                    zz = (z + k) % nz if d == 1 else (z + nz - k) % nz
                    self.across(zz, d).wait_recv()

                @pl.when(c == (1 if d == 1 else 0))
                def _():
                    self.across(z, d).wait_recv()
                    self.across((z + mid) % nz, d).wait_recv()

            elif d:
                for zz in range(nz):
                    self.across(zz, d).wait_recv()
            self.side(d).start()

        def finish_side(self):
            for d in range(NX):
                self.side(d).wait_recv()

        def finish_sends(self):
            for k in range(1, mid):
                self.up(z, k).wait_send()
                self.low(z, k).wait_send()

            @pl.when(c == 0)
            def _():
                self.up(z, mid).wait_send()

            @pl.when(c == 1)
            def _():
                self.low(z, mid).wait_send()

            for d in range(1, NX):
                for zz in range(nz):
                    self.across(zz, d).wait_send()
            for d in range(NX):
                self.side(d).wait_send()

    w_out = Weight(wo, 0)
    w_down = Weight(wd, 1)
    up_copy(mine, 0, 0).start()
    low_copy(mine, 0, 0).start()
    side_copy(mine, 0, 0).start()
    x_copies = {}
    for d in order[1:]:
        to = (x + d) % NX
        x_copies[d] = remote(
            packkv.at[to],
            kv.at[mine, :, my_rows, :],
            xs_sem.at[d - 1],
            xr_sem.at[d - 1],
            dev(z, to, c),
        )
        x_copies[d].start()
    q_copies = []
    for d in order[1:]:
        to = (x + d) % NX
        copy = remote(
            packq.at[to],
            qrecv.at[my_rows, :],
            xs_sem.at[NX + d - 2],
            xr_sem.at[NX + d - 2],
            dev(z, to, c),
        )
        copy.start()
        q_copies.append(copy)
    for s, d in enumerate(order[1:], 1):
        x_copies[d].wait_recv()
        up_copy(mine, s, s).start()
        low_copy(mine, s, s).start()
        side_copy(mine, s, s).start()

    loads[5].wait()
    w_out.begin()
    w_out.begin_across()
    acc[...] = jnp.zeros_like(acc)
    tot[...] = jnp.zeros_like(tot)
    mx[...] = jnp.full(mx.shape, -3e38, F32)
    for copy in q_copies:
        copy.wait_recv()
    lane = lax.broadcasted_iota(jnp.int32, (rows, 128), 1) < 64
    queries = qrecv[...].astype(F32)
    qs[0:rows, :] = jnp.where(lane, queries, 0.0).astype(BF16)
    qs[rows : 2 * rows, :] = jnp.where(lane, 0.0, queries).astype(BF16)
    loads[6].wait()

    scale = 64 ** (-0.5) * math.log2(math.e)
    tile = rows

    def attend(blocks):
        width = len(blocks) * tokens
        keys = jnp.concatenate([piece(slot, s)[0] for slot, s in blocks], axis=0)
        vals = jnp.concatenate([piece(slot, s)[1] for slot, s in blocks], axis=0)
        halves = [pl.ds(n * tile, tile) for n in range(2)]
        for at, scores in [(at, dot_nt(qs[at, :], keys)) for at in halves]:
            old = mx[at, :]
            top = scores[:, 0:128]
            for lo in range(128, width, 128):
                top = jnp.maximum(top, scores[:, lo : lo + 128])
            new = jnp.maximum(old, jnp.max(top, axis=1, keepdims=True))
            factor = jnp.exp2((old - new) * scale)
            total = tot[at, :] * factor
            parts = []
            for lo in range(0, width, 128):
                part = jnp.exp2((scores[:, lo : lo + 128] - new) * scale)
                total = total + part
                parts.append(part.astype(BF16))
            mx[at, :] = new
            tot[at, :] = total
            acc[at, :] = acc[at, :] * factor + jnp.dot(
                jnp.concatenate(parts, axis=1), vals, preferred_element_type=F32
            )

    attend([(mine, s) for s in range(NX)])

    def step(i, carry):
        below, below_s = from_below(i, c)
        above, above_s = from_above(i, c)
        up_copy(below, below_s, i).wait_recv()

        @pl.when(i == DOWN_AT)
        def _():
            w_down.begin()

        @pl.when((i > DOWN_AT) & ((i - DOWN_AT) % NX == 0))
        def _():
            w_down.relay((i - DOWN_AT) // NX)
            w_down.spread((i - DOWN_AT) // NX)

        @pl.when(i < steps - NX)
        def _():
            up_copy(below, below_s, i + NX).start()

        low_copy(above, above_s, i).wait_recv()

        @pl.when((i < steps - NX - half) | ((i >= steps - NX) & (i < steps - half)))
        def _():
            to = jnp.where(i < steps - NX - half, i + NX, i + half)
            low_copy(above, above_s, to).start()

        side_copy(below, below_s, NX + i).start()
        side_copy(above, above_s, NX + steps + i).start()

        @pl.when(i == DOWN_AT)
        def _():
            w_down.begin_across()

        @pl.when((i % 2 == 1) & (i < 2 * mid))
        def _():
            w_out.relay((i + 1) // 2)
            w_out.spread((i + 1) // 2)

        @pl.when((i % 2 == 1) & (i >= OUT_ON))
        def _():
            w_out.onward((i - OUT_ON) // 2)

        @pl.when((i > DOWN_AT) & ((i - DOWN_AT) % NX == 1) & (i >= DOWN_AT + NX))
        def _():
            w_down.onward((i - DOWN_AT) // NX - 1)

        other_b, other_bs = from_below(i - half, 1 - c)
        other_a, other_as = from_above(i - half, 1 - c)
        b_index = jnp.where(i < half, 2 * i, NX + i - half)
        a_index = jnp.where(i < half, 2 * i + 1, NX + steps + i - half)
        side_copy(other_b, other_bs, b_index).wait_recv()
        side_copy(other_a, other_as, a_index).wait_recv()
        attend([(below, below_s), (above, above_s), (other_b, other_bs), (other_a, other_as)])
        return carry

    lax.fori_loop(0, steps, step, 0)
    in_loop = (steps - 1 - DOWN_AT) // NX
    w_out.gather_side(0)
    for k in range((steps - 1 - steps % 2 - OUT_ON) // 2 + 1, mid + 1):
        w_out.onward(k)
    for k in range((steps - 2 - DOWN_AT) // NX, in_loop):
        w_down.onward(k)
    if in_loop < mid - 1:
        w_down.relay(in_loop + 1)
    last = []
    for j in range(steps - half, steps):
        b = from_below(j, 1 - c)
        a = from_above(j, 1 - c)
        side_copy(*b, NX + j).wait_recv()
        side_copy(*a, NX + steps + j).wait_recv()
        last += [b, a]
    for d in order[1:]:
        w_out.gather_side(d)
    attend(last)

    weight = lam_ref[x]
    for j in range(NX):
        a, b = j * tokens, rows + j * tokens
        first = acc[a : a + tokens, :] / jnp.sum(tot[a : a + tokens, :], axis=1, keepdims=True)
        second = acc[b : b + tokens, :] / jnp.sum(tot[b : b + tokens, :], axis=1, keepdims=True)
        diff = first - weight * second
        normal = diff * lax.rsqrt(jnp.mean(diff * diff, axis=1, keepdims=True) + EPS)
        asend[j] = (normal * hgain_ref[...]).astype(BF16)

    my_cols = pl.ds(pl.multiple_of(x * 128, 128), 128)
    a_copies = []
    for d in order[1:]:
        to = (x + d) % NX
        copy = remote(
            asend.at[to],
            arecv.at[:, my_cols],
            as_sem.at[d - 1],
            ar_sem.at[d - 1],
            dev(z, to, c),
        )
        copy.start()
        a_copies.append(copy)
    arecv[:, my_cols] = asend[x]
    if in_loop < mid - 1:
        w_down.spread(in_loop + 1)
    w_out.finish_side()
    for copy in a_copies:
        copy.wait()

    n_rows = res.shape[0]
    width = wo.shape[4]
    hidden_width = wd.shape[4]
    feature_rows = NX * NC * wo.shape[3]

    cols = wo.shape[0] * feature_rows // PARTS
    per_part = nz // PARTS

    def project(rows_ref, weights, k_width, send, recv, s_sem, r_sem):
        copies = []
        for p in range(PARTS):
            at = pl.ds(p * cols, cols)
            w = weights[p * per_part : (p + 1) * per_part].reshape(cols, k_width)
            part = dot_nt(rows_ref[...], w).astype(BF16)
            for t in range(n_tp):
                send[t, :, at] = part[t * n_rows : (t + 1) * n_rows, :]
            for d in range(1, n_tp):
                to = (tp + d) % n_tp
                n = p * (n_tp - 1) + d - 1
                copy = remote(
                    send.at[to, :, at],
                    recv.at[d - 1, :, at],
                    s_sem.at[n],
                    r_sem.at[n],
                    (sp, to),
                )
                copy.start()
                copies.append(copy)
        return copies

    copies = project(arecv, wo, width, psend, precv, ps_sem, pr_sem)
    for k in range(min(in_loop + 2, mid), mid + 1):
        w_down.relay(k)
        w_down.spread(k)
    for k in range(in_loop, mid):
        w_down.onward(k)
    loads[9].wait()
    total = psend[tp].astype(F32)
    for copy in copies:
        copy.wait()
    for d in range(n_tp - 1):
        total = total + precv[d].astype(F32)
    summed = (res[...].astype(F32) + total).astype(BF16)
    after[...] = summed
    stream = summed.astype(F32)
    normal = stream * lax.rsqrt(jnp.mean(stream * stream, axis=1, keepdims=True) + EPS)
    normed = (normal * ngain_ref[...]).astype(BF16)
    nsend[...] = normed
    my_part = pl.ds(pl.multiple_of(tp * n_rows, n_rows), n_rows)
    copies = []
    middle = nsend.shape[1] // 2
    sides = (pl.ds(0, middle), pl.ds(middle, middle))
    for n, side in enumerate(sides):
        for d in range(1, n_tp):
            copy = remote(
                nsend.at[:, side],
                shard.at[my_part, side],
                ns_sem.at[n * (n_tp - 1) + d - 1],
                nr_sem.at[n * (n_tp - 1) + d - 1],
                (sp, (tp + d) % n_tp),
            )
            copy.start()
            copies.append(copy)
    shard[my_part, :] = normed
    w_down.gather_side(0)
    w_down.onward(mid)
    loads[7].wait()
    loads[8].wait()
    tiles = [(lo, min(lo + 256, hidden_width)) for lo in range(0, hidden_width, 256)]
    for copy in copies[: n_tp - 1]:
        copy.wait()
    for lo, hi in tiles:
        left = shard[:, 0:middle]
        gacc[:, lo:hi] = jnp.dot(left, gv[0:middle, lo:hi], preferred_element_type=F32)
        uacc[:, lo:hi] = jnp.dot(left, uv[0:middle, lo:hi], preferred_element_type=F32)
    for copy in copies[n_tp - 1 :]:
        copy.wait()
    w_down.gather_side(1)
    w_down.gather_side(NX - 1)
    for lo, hi in tiles:
        left = shard[:, middle:]
        gate = gacc[:, lo:hi] + jnp.dot(left, gv[middle:, lo:hi], preferred_element_type=F32)
        up = uacc[:, lo:hi] + jnp.dot(left, uv[middle:, lo:hi], preferred_element_type=F32)
        hid[:, lo:hi] = (gate / (1.0 + jnp.exp(-gate)) * up).astype(BF16)
    for d in range(2, NX - 1):
        w_down.gather_side(d)
    w_down.finish_side()

    copies = project(hid, wd, hidden_width, dsend, drecv, fs_sem, fr_sem)

    for d in range(1, NX):
        x_copies[d].wait_send()
    for copy in q_copies:
        copy.wait_send()
    for n in range(steps):
        up_copy(mine, 0, n).wait_send()
        low_copy(mine, 0, n).wait_send()
    for n in range(NX + 2 * steps):
        side_copy(mine, 0, n).wait_send()
    w_out.finish_sends()
    w_down.finish_sends()

    total = dsend[tp].astype(F32)
    for copy in copies:
        copy.wait()
    for d in range(n_tp - 1):
        total = total + drecv[d].astype(F32)
    out_ref[...] = (after[...].astype(F32) + total).astype(BF16)


def local(nz, n_tp, residual, q1, k1, q2, k2, v, lam, head_gain, out_w, norm_gain, gate, up, down):
    tokens = q1.shape[0]
    rows = NX * tokens
    n_rows, features = residual.shape
    hidden = gate.shape[1]
    steps = NX * (nz - 1) // 2
    mid = nz // 2
    vmem = pl.BlockSpec(memory_space=pltpu.VMEM)
    smem = pl.BlockSpec(memory_space=pltpu.SMEM)
    hbm = pl.BlockSpec(memory_space=pl.ANY)
    dma = pltpu.SemaphoreType.DMA

    def like(a):
        return pltpu.VMEM(a.shape, a.dtype)

    return pl.pallas_call(
        functools.partial(kernel, nz, n_tp),
        out_shape=jax.ShapeDtypeStruct((n_rows, features), BF16),
        in_specs=[hbm] * 6 + [smem, vmem, hbm, vmem, hbm, hbm, hbm],
        out_specs=vmem,
        scratch_shapes=[
            like(residual),
            like(q1),
            like(k1),
            like(q2),
            like(k2),
            like(v),
            like(gate),
            like(up),
            pltpu.VMEM((nz, NX, NC, *out_w.shape), BF16),
            pltpu.VMEM((nz, NX, NC, *down.shape), BF16),
            pltpu.VMEM((NX, tokens, 128), BF16),
            pltpu.VMEM((NX, 2, tokens, 128), BF16),
            pltpu.VMEM((rows, 128), BF16),
            pltpu.VMEM((2 * rows, 128), BF16),
            pltpu.VMEM((nz * NC, 2, rows, 128), BF16),
            pltpu.VMEM((2 * rows, 128), F32),
            pltpu.VMEM((2 * rows, 128), F32),
            pltpu.VMEM((2 * rows, 128), F32),
            pltpu.VMEM((NX, tokens, 128), BF16),
            pltpu.VMEM((tokens, NX * 128), BF16),
            pltpu.VMEM((n_tp, n_rows, features), BF16),
            pltpu.VMEM((n_tp - 1, n_rows, features), BF16),
            pltpu.VMEM((n_rows, features), BF16),
            pltpu.VMEM((n_rows, features), BF16),
            pltpu.VMEM((tokens, features), BF16),
            pltpu.VMEM((tokens, hidden), F32),
            pltpu.VMEM((tokens, hidden), F32),
            pltpu.VMEM((tokens, hidden), BF16),
            pltpu.VMEM((n_tp, n_rows, features), BF16),
            pltpu.VMEM((n_tp - 1, n_rows, features), BF16),
            dma((10,)),
            dma((2 * (NX - 1),)),
            dma((2 * (NX - 1),)),
            dma((steps,)),
            dma((steps,)),
            dma((steps,)),
            dma((steps,)),
            dma((NX + 2 * steps,)),
            dma((NX + 2 * steps,)),
            dma((NX - 1,)),
            dma((NX - 1,)),
            dma((2 * mid,)),
            dma((2 * mid,)),
            dma((2 * mid,)),
            dma((2 * mid,)),
            dma((2 * (NX - 1) * nz,)),
            dma((2 * (NX - 1) * nz,)),
            dma((2 * NX,)),
            dma((2 * NX,)),
            dma((PARTS * (n_tp - 1),)),
            dma((PARTS * (n_tp - 1),)),
            dma((2 * (n_tp - 1),)),
            dma((2 * (n_tp - 1),)),
            dma((PARTS * (n_tp - 1),)),
            dma((PARTS * (n_tp - 1),)),
        ],
        compiler_params=pltpu.CompilerParams(
            collective_id=0, has_side_effects=True, vmem_limit_bytes=62 * 2**20
        ),
        name="layer",
    )(
        residual,
        q1,
        k1,
        q2,
        k2,
        v,
        lam,
        head_gain.reshape(1, 128),
        out_w,
        norm_gain.reshape(1, features),
        gate,
        up,
        down,
    )


def solution(mesh):
    nz = mesh.shape["sp"] // (NX * NC)
    n_tp = mesh.shape["tp"]
    return jax.shard_map(
        functools.partial(local, nz, n_tp),
        mesh=mesh,
        in_specs=(
            P(("sp", "tp"), None),
            P("sp", "tp"),
            P("sp", "tp"),
            P("sp", "tp"),
            P("sp", "tp"),
            P("sp", "tp"),
            P("tp"),
            P(),
            P("sp", "tp"),
            P(),
            P(None, "tp"),
            P(None, "tp"),
            P("sp", "tp"),
        ),
        out_specs=P(("sp", "tp"), None),
        check_vma=False,
    )
```
